256 devices in a mesh: sp: 64 (over z, y, core), tp: 4 (over x).
Axes of the slice: x: 4, y: 4, z: 8, core: 2. Of those that a mesh axis runs over, the one named last changes fastest.
Arguments:
- mixer_out: bfloat16 [8192, 2048], P('sp'), may hold values from -6 to 6
- conv_out: bfloat16 [8192, 2048], P('sp', 'tp'), may hold values from -350 to 350
- out_cot: bfloat16 [8192, 2048], P('sp'), may hold values from -16 to 16
- routes: int32 [8192, 2], P('sp'), may hold values from 0 to 63, all different within a row; in each aligned block of 128 rows (0 to 127, 128 to 255, ...) at most 8 rows name the same one
- route_weight: float32 [8192, 2], P('sp'), may hold values from 0.3 to 2.5
- gate_weight: bfloat16 [64, 2048, 1024], P('sp', None, 'tp'), may hold values from -0.125 to 0.125
- up_weight: bfloat16 [64, 2048, 1024], P('sp', None, 'tp'), may hold values from -0.125 to 0.125
- down_weight: bfloat16 [64, 1024, 2048], P('sp', 'tp'), may hold values from -0.1875 to 0.1875
- out_weight: bfloat16 [2048, 2048], P('tp'), may hold values from -0.125 to 0.125
- norm_gain: float32 [2048], P('tp'), may hold values from 0.1 to 1.9
- conv_taps: float32 [31, 2048], P(None, 'tp'), may hold values from -1 to 1
Outputs:
- gate_grad: bfloat16 [64, 2048, 1024], P('sp', None, 'tp')
- up_grad: bfloat16 [64, 2048, 1024], P('sp', None, 'tp')
- down_grad: bfloat16 [64, 1024, 2048], P('sp', 'tp')
- proj_grad: float32 [2048, 2048], P('sp', 'tp')
- gated_grad: float32 [8192, 2048], P('sp', 'tp')
The draws below stay inside these ranges and needn't reach their ends.
Inputs may be any that keep to these rules, and one draw needn't show every extreme that they name: `routes`: each row names 2 different experts. Among the rows of one device no expert is named by more than 8 rows, and in every draw some expert is named by exactly 8 rows of some device.
All inputs are finite; a program needn't handle non-finite values.
Results may differ from the reference program's by a relative error of at most 0.0095.
Values may be sent and summed in bfloat16 or wider, within the bound.
No kernel may reach another device: no remote copies, remote signals or barrier semaphores. Data moves between devices by JAX's collectives and lax.ppermute only.
A program may use at most 64 MiB of HBM per device.

```python
import math
import jax
import jax.numpy as jnp
import numpy as np
from jax import lax

D = 2048
FE = 1024
KW = 31
TOP = 2
TOK_DEV = 128
TOKENS = 8192
EXPERTS = 64
CAP = 8
N_SP = 64
N_TP = 4


def draw_conv_out(key, part):
    keys = jax.random.split(key, 3)
    column = jnp.exp(jnp.log(3.0) * jnp.arange(D, dtype=jnp.float32) / (D - 1))
    column = column * jnp.exp(jax.random.uniform(keys[2], (1, D), jnp.float32, -0.35, 0.35))
    base = jnp.clip(jax.random.normal(keys[0], (TOKENS, D), jnp.float32), -5.0, 5.0)
    row_scale = jnp.exp(jax.random.uniform(keys[1], (TOKENS, 1), jnp.float32) * jnp.log(10.0))
    return (base * row_scale * column).astype(jnp.bfloat16)


def strengthened(drawn, rng, source, target, blocks, factor):
    owner, partner = [(jnp.arange(drawn.shape[dim]) // (drawn.shape[dim] // blocks)).reshape([-1 if axis == dim else 1 for axis in range(drawn.ndim)]) for dim in (source, target)]
    chosen = jax.random.permutation(rng, blocks)[partner]
    strong = (owner == chosen) | (owner == (partner + blocks // 2) % blocks)
    return jnp.where(strong, factor * drawn, drawn)


def levels(stream_key, extent, pieces, smallest, largest):
    def one(dim, blocks):
        steps = jax.random.uniform(jax.random.fold_in(jax.random.fold_in(stream_key, 6), dim), (blocks,), jnp.float32, smallest / len(pieces), largest / len(pieces))
        return jnp.repeat(jnp.exp(steps), extent[dim] // blocks).reshape((-1,) + (1,) * (len(extent) - dim - 1))

    gain = one(*pieces[0])
    for cut in pieces[1:]:
        gain = gain * one(*cut)
    return gain


def deal_out(own_key, own, number, rows, amount, top, limit, skew):
    ranking = jax.random.permutation(own_key, amount)
    packed, usual = portions_of(amount, rows * top, limit, skew, True), portions_of(amount, rows * top, limit, skew, False)
    places = jnp.arange(amount)

    def named(tallies, turn):
        used = int((tallies > 0).sum())
        fixed = max(1, used // 4)
        moved = fixed + (places - fixed + turn * (used - fixed)) % max(1, amount - fixed)
        return jnp.zeros((amount,), jnp.int32).at[ranking[jnp.where(places < fixed, places, moved)]].set(jnp.asarray(tallies, jnp.int32))

    tallies = jnp.where(number % 4 == 0, named(packed, number // 4), named(usual, number - number // 4 - 1))
    mixed = jax.random.permutation(jax.random.fold_in(own, 3), amount)
    giver, taker = mixed[0:amount // 2 * 2:2], mixed[1:amount // 2 * 2:2]
    room = jnp.minimum(tallies[giver] - 1, limit - tallies[taker]) // 2
    room = jnp.where((giver == ranking[0]) | (taker == ranking[0]) | (tallies[taker] == 0), 0, jnp.maximum(room, 0))
    moved = jax.random.randint(jax.random.fold_in(own, 4), (amount // 2,), 0, 1 << 20) % (room + 1)
    tallies = tallies.at[giver].add(-moved).at[taker].add(moved)
    items = jnp.searchsorted(jnp.cumsum(tallies), jnp.arange(rows * top), side="right").astype(jnp.int32)
    listing = items.reshape(top, rows).T
    listing = listing[jax.random.permutation(jax.random.fold_in(own, 1), rows)]
    turn = jax.random.randint(jax.random.fold_in(own, 2), (rows, 1), 0, top)
    return jnp.take_along_axis(listing, (jnp.arange(top)[None, :] + turn) % top, axis=1)


def portions_of(number_of, total, most, skew, full):
    weights = [(1 << 20) // math.isqrt(grade ** skew) + 1 for grade in range(1, number_of + 1)]
    largest = most if full else min(most, max(-(-total // number_of), total * weights[0] // sum(weights)))
    least = 1 if total - largest >= number_of - 1 else 0
    given, surplus = [largest] + [least] * (number_of - 1), total - largest - least * (number_of - 1)
    while surplus > 0:
        free = [i for i in range(1, number_of) if given[i] < largest] or [i for i in range(1, number_of) if given[i] < most]
        pool, left = sum([weights[i] for i in free]), surplus
        for i in free:
            more = min(most - given[i], max(1, left * weights[i] // pool), surplus)
            given[i] = given[i] + more
            surplus = surplus - more
    return np.array(given)


def centred(stream_key, shape, deviation, most, pieces=(), held_as=jnp.bfloat16):
    values = deviation * jax.random.normal(stream_key, shape, jnp.float32)
    if pieces:
        values = values * levels(stream_key, shape, pieces, -0.22, 0.18)
    return jnp.clip(values, -most, most).astype(held_as)


def noise_with(stream_key, shape, deviation, most, pieces, heavy, kind=jnp.bfloat16):
    array = deviation * jax.random.normal(stream_key, shape, jnp.float32)
    if pieces:
        array = array * levels(stream_key, shape, pieces, -0.22, 0.18)
    return jnp.clip(strengthened(array, jax.random.fold_in(stream_key, 3), *heavy), -most, most).astype(kind)


def setup_inputs(seed: int = 0) -> dict:
    arg_keys = jax.random.split(jax.random.key(seed), 12)
    mixer_out = centred(arg_keys[0], (TOKENS, D), 1.0, 6.0, ((0, 64),))
    conv_out = draw_conv_out(jax.random.fold_in(arg_keys[11], 71), 0)
    out_cot = noise_with(arg_keys[2], (TOKENS, D), 1.0, 16.0, ((0, 64),), (0, 1, 64, 4.0))
    routes_keys = jax.random.split(jax.random.fold_in(arg_keys[3], 1), TOKENS // TOK_DEV)
    routes_turns = jax.random.permutation(jax.random.fold_in(arg_keys[3], 3), TOKENS // TOK_DEV)
    routes = jax.vmap(lambda own, number: deal_out(jax.random.fold_in(arg_keys[3], 2), own, number, TOK_DEV, EXPERTS, TOP, CAP, 2))(routes_keys, routes_turns).reshape((TOKENS, TOP))
    route_weight = jnp.clip(jnp.exp(math.log(2.5) - 2.1202635 * jax.random.uniform(arg_keys[4], (TOKENS, TOP), jnp.float32) ** levels(arg_keys[4], (TOKENS, TOP), ((0, 64),), -0.2, 0.2)), 0.3, 2.5)
    gate_weight = centred(arg_keys[5], (EXPERTS, D, FE), D ** -0.5, 0.125, ((0, 64), (2, 4)))
    up_weight = centred(arg_keys[6], (EXPERTS, D, FE), D ** -0.5, 0.125, ((0, 64), (2, 4)))
    down_weight = centred(arg_keys[7], (EXPERTS, FE, D), FE ** -0.5, 0.1875, ((0, 64), (1, 4)))
    out_weight = centred(arg_keys[8], (D, D), D ** -0.5, 0.125, ((0, 4),))
    norm_gain = jnp.clip(1.0 + 0.18 * jax.random.normal(arg_keys[9], (D,), jnp.float32), 0.1, 1.9)
    conv_taps = centred(arg_keys[10], (KW, D), KW ** -0.5, 1.0, ((1, 4),), jnp.float32)
    return {"mixer_out": mixer_out, "conv_out": conv_out, "out_cot": out_cot, "routes": routes, "route_weight": route_weight, "gate_weight": gate_weight, "up_weight": up_weight, "down_weight": down_weight, "out_weight": out_weight, "norm_gain": norm_gain, "conv_taps": conv_taps}


norm_epsilon = 1e-05

def expert_backward(x_rows, cot_rows, w_gate, w_up, w_down, parts):
    pre_gate = jnp.dot(x_rows, w_gate, preferred_element_type=jnp.float32)
    pre_up = jnp.dot(x_rows, w_up, preferred_element_type=jnp.float32)
    sig_gate = jax.nn.sigmoid(pre_gate)
    activation = (pre_gate * sig_gate * pre_up).astype(jnp.bfloat16)
    down_g = lax.dot_general(activation, cot_rows, (((0,), (0,)), ((), ())), preferred_element_type=jnp.float32).astype(jnp.bfloat16)
    act_grad = lax.dot_general(cot_rows, w_down, (((1,), (1,)), ((), ())), preferred_element_type=jnp.float32)
    gate_pre_grad = (act_grad * pre_up * sig_gate * (1.0 + pre_gate * (1.0 - sig_gate))).astype(jnp.bfloat16)
    up_pre_grad = (act_grad * pre_gate * sig_gate).astype(jnp.bfloat16)
    gate_g = lax.dot_general(x_rows, gate_pre_grad, (((0,), (0,)), ((), ())), preferred_element_type=jnp.float32).astype(jnp.bfloat16)
    up_g = lax.dot_general(x_rows, up_pre_grad, (((0,), (0,)), ((), ())), preferred_element_type=jnp.float32).astype(jnp.bfloat16)
    part_width = w_gate.shape[1] // parts
    total_back = jnp.zeros((x_rows.shape[0], w_gate.shape[0]), jnp.float32)
    for part_index in range(parts):
        lower = part_index * part_width
        upper = lower + part_width
        partial_value = lax.dot_general(gate_pre_grad[:, lower:upper], w_gate[:, lower:upper], (((1,), (1,)), ((), ())), preferred_element_type=jnp.float32)
        partial_value = partial_value + lax.dot_general(up_pre_grad[:, lower:upper], w_up[:, lower:upper], (((1,), (1,)), ((), ())), preferred_element_type=jnp.float32)
        rounded = lax.optimization_barrier(partial_value.astype(jnp.bfloat16))
        total_back = total_back + rounded.astype(jnp.float32)
    return (gate_g, up_g, down_g, total_back)

def reference(mixer_out, conv_out, out_cot, routes, route_weight, gate_weight, up_weight, down_weight, out_weight, norm_gain, conv_taps):
    entries = TOKENS * TOP
    flat_routes = routes.reshape(-1).astype(jnp.int32)
    one_hot = (flat_routes[:, None] == jnp.arange(EXPERTS, dtype=jnp.int32)[None, :]).astype(jnp.int32)
    by_source = one_hot.reshape(N_SP, TOK_DEV * TOP, EXPERTS)
    earlier = jnp.cumsum(by_source, axis=1) - by_source
    within = lax.optimization_barrier(jnp.sum(earlier * by_source, axis=2)).reshape(-1)
    source_index = jnp.arange(entries, dtype=jnp.int32) // (TOK_DEV * TOP)
    slot_index = (source_index * CAP + within).astype(jnp.int32)
    table = jnp.full((EXPERTS, N_SP * CAP), entries, jnp.int32)
    table = table.at[flat_routes, slot_index].set(jnp.arange(entries, dtype=jnp.int32))
    weights_flat = route_weight.reshape(-1)

    def per_expert(carry, inputs):
        w_gate, w_up, w_down, entry_ids = inputs
        token_ids = (entry_ids // TOP).astype(jnp.int32)
        x_rows = jnp.take(mixer_out, token_ids, axis=0, mode='fill', fill_value=0)
        cot_rows = jnp.take(out_cot, token_ids, axis=0, mode='fill', fill_value=0)
        scale_rows = jnp.take(weights_flat, entry_ids, axis=0, mode='fill', fill_value=0)
        row_cot = (scale_rows[:, None] * cot_rows.astype(jnp.float32)).astype(jnp.bfloat16)
        gate_g, up_g, down_g, total_back = expert_backward(x_rows, row_cot, w_gate, w_up, w_down, N_TP)
        row_back = lax.optimization_barrier(total_back.astype(jnp.bfloat16))
        carry = carry.at[token_ids].add(row_back.astype(jnp.float32), mode='drop')
        return (carry, (gate_g, up_g, down_g))
    summed, stacked = lax.scan(per_expert, out_cot.astype(jnp.float32), (gate_weight, up_weight, down_weight, table))
    gate_grad, up_grad, down_grad = stacked
    mix_grad = summed.astype(jnp.bfloat16)
    conv_vals = conv_out.astype(jnp.float32)
    inv_rms = lax.rsqrt(lax.optimization_barrier(jnp.mean(conv_vals * conv_vals, axis=1, keepdims=True)) + norm_epsilon)
    normed = conv_vals * inv_rms * norm_gain[None, :]
    sig_norm = jax.nn.sigmoid(normed)
    activated = (normed * sig_norm).astype(jnp.bfloat16)
    proj_grad = lax.dot_general(mix_grad, activated, (((0,), (0,)), ((), ())), preferred_element_type=jnp.float32)
    norm_in_grad = lax.dot_general(mix_grad, out_weight, (((1,), (1,)), ((), ())), preferred_element_type=jnp.float32)
    scaled = norm_in_grad * sig_norm * (1.0 + normed * (1.0 - sig_norm)) * norm_gain[None, :]
    conv_grad = inv_rms * scaled - conv_vals * inv_rms ** 3 * lax.optimization_barrier(jnp.mean(conv_vals * scaled, axis=1, keepdims=True))
    padded = jnp.pad(conv_grad, ((0, KW - 1), (0, 0)))
    gated_grad = jnp.zeros((TOKENS, D), jnp.float32)
    for tap_index in range(KW):
        gated_grad = gated_grad + conv_taps[tap_index][None, :] * padded[tap_index:tap_index + TOKENS]
    return (gate_grad, up_grad, down_grad, proj_grad, gated_grad)
```

```python
import functools

import jax
import jax.numpy as jnp
from jax import lax
from jax.experimental import pallas as pl
from jax.experimental.pallas import tpu as pltpu
from jax.sharding import Mesh
from jax.sharding import PartitionSpec as P


norm_epsilon = 1e-05
SP = ("z", "y", "core")
f32 = jnp.float32
bf16 = jnp.bfloat16
VM = pl.BlockSpec(memory_space=pltpu.VMEM)
SM = pl.BlockSpec(memory_space=pltpu.SMEM)


def cost(flops, moved):
    return pl.CostEstimate(flops=flops, bytes_accessed=moved, transcendentals=0)


def dot(a, b, ca, cb):
    return lax.dot_general(a, b, (((ca,), (cb,)), ((), ())), preferred_element_type=f32)


def send_kernel(tp_ref, routes_ref, weight_ref, x_ref, cot_ref, sx_ref, sc_ref, sel_ref):
    tokens = routes_ref.shape[1]
    slots = sel_ref.shape[0]
    experts = sx_ref.shape[0]
    capacity = slots // experts
    expert_row = lax.broadcasted_iota(jnp.int32, (experts, tokens), 0)
    earlier = (
        lax.broadcasted_iota(jnp.int32, (tokens, tokens), 0)
        < lax.broadcasted_iota(jnp.int32, (tokens, tokens), 1)
    ).astype(bf16)
    slot_row = lax.broadcasted_iota(jnp.int32, (slots, tokens), 0)
    total = jnp.zeros((experts, 1), f32)
    picks = []
    for k in range(routes_ref.shape[0]):
        named = routes_ref[k : k + 1, :]
        hot = (expert_row == named).astype(f32)
        before = dot(hot.astype(bf16), earlier, 1, 0) + total
        total = total + jnp.sum(hot, axis=1, keepdims=True)
        within = jnp.sum(hot * before, axis=0, keepdims=True).astype(jnp.int32)
        picks.append((slot_row == named * capacity + within).astype(bf16))
    both = picks[0] + picks[1]
    sel_ref[...] = both
    shape = sx_ref.shape
    sx_ref[...] = dot(both, x_ref[...], 1, 0).astype(bf16).reshape(shape)
    cot = cot_ref[...].astype(f32)
    scaled = [(weight_ref[:, k : k + 1] * cot).astype(bf16) for k in range(2)]
    out = dot(picks[0], scaled[0], 1, 0) + dot(picks[1], scaled[1], 1, 0)
    sc_ref[...] = out.astype(bf16).reshape(shape)


def send_rows(tp, routes, route_weight, mixer_out, out_cot, experts, capacity, quarter):
    tokens = out_cot.shape[0]
    column = pl.BlockSpec((tokens, quarter), lambda i, t: (0, t[0]))
    whole = lambda shape: pl.BlockSpec(shape, lambda i, t: (0,) * len(shape))
    sent = jax.ShapeDtypeStruct((experts, capacity, quarter), bf16)
    return pl.pallas_call(
        send_kernel,
        grid_spec=pltpu.PrefetchScalarGridSpec(
            num_scalar_prefetch=1,
            grid=(1,),
            in_specs=[whole((2, tokens)), whole((tokens, 2)), column, column],
            out_specs=[whole(sent.shape), whole(sent.shape), whole((experts * capacity, tokens))],
        ),
        out_shape=[sent, sent, jax.ShapeDtypeStruct((experts * capacity, tokens), bf16)],
        cost_estimate=cost(400_000_000, 3_000_000),
    )(tp, routes.T, route_weight, mixer_out, out_cot)


def block_of(t, k):
    return lax.rem(t + k, 4)


def forward_kernel(t_ref, *refs):
    blocks, (wg_ref, wu_ref, pg_ref, pu_ref) = refs[:8], refs[8:]
    half, width = blocks[0].shape
    for h in range(2):
        rows = pl.ds(h * half, half)
        for w_ref, o_ref in ((wg_ref, pg_ref), (wu_ref, pu_ref)):
            acc = None
            for k in range(4):
                at = pl.multiple_of(block_of(t_ref[0], k) * width, width)
                part = dot(blocks[2 * k + h][...], w_ref[pl.ds(at, width), :], 1, 0)
                acc = part if acc is None else acc + part
            o_ref[rows, :] = acc


def expert_forward(tp, x_blocks, w_gate, w_up):
    rows, hidden = 2 * x_blocks[0].shape[0], w_gate.shape[1]
    out = jax.ShapeDtypeStruct((rows, hidden), f32)
    return pl.pallas_call(
        forward_kernel,
        in_specs=[SM] + [VM] * 10,
        out_specs=[VM, VM],
        out_shape=[out, out],
        cost_estimate=cost(1_073_741_824, 5_000_000),
    )(tp, *x_blocks, w_gate, w_up)


def backward_kernel(t_ref, *refs):
    blocks = refs[:8]
    wd_ref, pg_ref, pu_ref, wg_ref, wu_ref, act_ref, gp_ref, up_ref, part_ref = refs[8:]
    half, width = blocks[0].shape
    for h in range(2):
        rows = pl.ds(h * half, half)
        act_grad = None
        for k in range(4):
            at = pl.multiple_of(block_of(t_ref[0], k) * width, width)
            part = dot(blocks[2 * k + h][...], wd_ref[:, pl.ds(at, width)], 1, 1)
            act_grad = part if act_grad is None else act_grad + part
        pre_gate = pg_ref[rows, :]
        pre_up = pu_ref[rows, :]
        sig = jax.nn.sigmoid(pre_gate)
        silu = pre_gate * sig
        act_ref[rows, :] = (silu * pre_up).astype(bf16)
        gate_pre = (act_grad * pre_up * sig * (1.0 + pre_gate * (1.0 - sig))).astype(bf16)
        up_pre = (act_grad * silu).astype(bf16)
        gp_ref[rows, :] = gate_pre
        up_ref[rows, :] = up_pre
        for j in range(4):
            cols = pl.ds(j * width, width)
            back = dot(gate_pre, wg_ref[cols, :], 1, 1) + dot(up_pre, wu_ref[cols, :], 1, 1)
            part_ref[j, rows, :] = back.astype(bf16)


def expert_backward(tp, c_blocks, w_down, pre_gate, pre_up, w_gate, w_up):
    half, width = c_blocks[0].shape
    rows, hidden = pre_gate.shape
    small = jax.ShapeDtypeStruct((rows, hidden), bf16)
    return pl.pallas_call(
        backward_kernel,
        in_specs=[SM] + [VM] * 13,
        out_specs=[VM] * 4,
        out_shape=[small, small, small, jax.ShapeDtypeStruct((4, rows, width), bf16)],
        cost_estimate=cost(1_610_612_736, 9_000_000),
    )(tp, *c_blocks, w_down, pre_gate, pre_up, w_gate, w_up)


def weight_kernel(t_ref, *refs):
    xs, cs = refs[:8], refs[8:16]
    act_ref, gp_ref, up_ref, gg_ref, ug_ref, dg_ref = refs[16:]
    half, width = xs[0].shape
    top, low = pl.ds(0, half), pl.ds(half, half)
    for k in range(4):
        at = pl.ds(pl.multiple_of(block_of(t_ref[0], k) * width, width), width)
        a, b = xs[2 * k][...], xs[2 * k + 1][...]
        gg_ref[at, :] = (dot(a, gp_ref[top, :], 0, 0) + dot(b, gp_ref[low, :], 0, 0)).astype(bf16)
        ug_ref[at, :] = (dot(a, up_ref[top, :], 0, 0) + dot(b, up_ref[low, :], 0, 0)).astype(bf16)
        c, d = cs[2 * k][...], cs[2 * k + 1][...]
        down = dot(act_ref[top, :], c, 0, 0) + dot(act_ref[low, :], d, 0, 0)
        dg_ref[:, at] = down.astype(bf16)


def weight_grads(tp, x_blocks, c_blocks, act, gate_pre, up_pre):
    width = x_blocks[0].shape[1]
    hidden = act.shape[1]
    tall = jax.ShapeDtypeStruct((4 * width, hidden), bf16)
    return pl.pallas_call(
        weight_kernel,
        in_specs=[SM] + [VM] * 19,
        out_specs=[VM] * 3,
        out_shape=[tall, tall, jax.ShapeDtypeStruct((hidden, 4 * width), bf16)],
        cost_estimate=cost(1_610_612_736, 8_000_000),
    )(tp, *x_blocks, *c_blocks, act, gate_pre, up_pre)


def mix_kernel(t_ref, sel_ref, back_ref, cot_ref, mix_ref, out_ref):
    tokens, width = cot_ref.shape
    ret = back_ref[...].reshape(sel_ref.shape[0], width)
    mix = cot_ref[...].astype(f32) + dot(sel_ref[...], ret, 0, 0)
    for j in range(4):
        mix_ref[j] = mix.astype(bf16)
    turned = mix.T.astype(bf16)
    run = width // 16
    for g in range(8):
        piece = jnp.concatenate(
            [turned[(q * 8 + g) * run : (q * 8 + g + 1) * run] for q in range(2)], axis=0
        )
        for j in range(4):
            out_ref[g * 4 + j] = piece


def mix_parts(tp, sel, returned, out_cot):
    tokens = out_cot.shape[0]
    experts, capacity, quarter = returned.shape
    whole = lambda shape: pl.BlockSpec(shape, lambda i, t: (0,) * len(shape))
    shapes = [(4, tokens, quarter), (32, quarter // 8, tokens)]
    return pl.pallas_call(
        mix_kernel,
        grid_spec=pltpu.PrefetchScalarGridSpec(
            num_scalar_prefetch=1,
            grid=(1,),
            in_specs=[
                whole(sel.shape),
                whole(returned.shape),
                pl.BlockSpec((tokens, quarter), lambda i, t: (0, t[0])),
            ],
            out_specs=[whole(s) for s in shapes],
        ),
        out_shape=[jax.ShapeDtypeStruct(s, bf16) for s in shapes],
        cost_estimate=cost(70_000_000, 2_000_000),
    )(tp, sel, returned, out_cot)


def proj_kernel(mix_ref, act_ref, out_ref):
    groups, rows, tokens = mix_ref.shape[0] // 4, 4 * mix_ref.shape[1], mix_ref.shape[2]
    acc = None
    for g in range(groups):
        lhs = mix_ref[4 * g : 4 * g + 4].reshape(rows, tokens)
        part = dot(lhs, act_ref[g], 1, 0)
        acc = part if acc is None else acc + part
    out_ref[...] = acc.astype(bf16).reshape(out_ref.shape)


def proj_partial(mixed, activated):
    shape = (8, 4 * mixed.shape[1] // 8, activated.shape[2])
    return pl.pallas_call(
        proj_kernel,
        in_specs=[VM, VM],
        out_specs=VM,
        out_shape=jax.ShapeDtypeStruct(shape, bf16),
        cost_estimate=cost(268_435_456, 2_000_000),
    )(mixed, activated)


def exchange(x, axis):
    return lax.all_to_all(x, axis, split_axis=0, concat_axis=0, tiled=True)


def from_everyone(x, axis):
    return exchange(jnp.broadcast_to(x, (lax.axis_size(axis), *x.shape)), axis)


def ring_gather(block):
    ring = range(4)
    ahead = [(i, (i + 1) % 4) for i in ring]
    behind = [(i, (i - 1) % 4) for i in ring]
    half = block.shape[0] // 2
    own = (block[:half], block[half:])
    ahead_a = lax.ppermute(own[0], "tp", ahead)
    behind_b = lax.ppermute(own[1], "tp", behind)
    ahead_b = lax.ppermute(own[1], "tp", ahead)
    behind_a = lax.ppermute(own[0], "tp", behind)
    across_a = lax.ppermute(ahead_a, "tp", ahead)
    across_b = lax.ppermute(behind_b, "tp", behind)
    return [*own, behind_a, behind_b, across_a, across_b, ahead_a, ahead_b]


def on_device(
    mixer_out,
    conv_out,
    out_cot,
    routes,
    route_weight,
    gate_weight,
    up_weight,
    down_weight,
    out_weight,
    norm_gain,
    conv_taps,
):
    tokens_here, model_width = out_cot.shape
    experts = lax.axis_size(SP)
    capacity = 2 * tokens_here * routes.shape[1] // experts
    quarter = conv_out.shape[1]
    tp = lax.axis_index("tp").astype(jnp.int32)[None]
    w_gate, w_up, w_down = gate_weight[0], up_weight[0], down_weight[0]

    send_x, send_cot, sel = send_rows(
        tp, routes, route_weight, mixer_out, out_cot, experts, capacity, quarter
    )
    slots = experts * capacity
    x_slice = exchange(send_x, SP).reshape(slots, quarter)
    cot_slice = exchange(send_cot, SP).reshape(slots, quarter)

    conv_vals = conv_out.astype(f32)
    power_sum = from_everyone(jnp.sum(conv_vals * conv_vals, axis=1)[None], "tp").sum(axis=(0, 1))
    inv_rms = lax.rsqrt(power_sum / model_width + norm_epsilon)[:, None]
    normed = conv_vals * inv_rms * norm_gain[None, :]
    sig_norm = jax.nn.sigmoid(normed)
    activated = (normed * sig_norm).astype(bf16)
    act_near = from_everyone(activated, ("y", "core"))

    x_blocks = ring_gather(x_slice)
    pre_gate, pre_up = expert_forward(tp, x_blocks, w_gate, w_up)
    c_blocks = ring_gather(cot_slice)
    act, gate_pre, up_pre, parts = expert_backward(
        tp, c_blocks, w_down, pre_gate, pre_up, w_gate, w_up
    )
    back = jnp.sum(exchange(parts, "tp").astype(f32), axis=0).astype(bf16)
    returned = exchange(back.reshape(experts, capacity, quarter), SP)
    gate_g, up_g, down_g = weight_grads(tp, x_blocks, c_blocks, act, gate_pre, up_pre)

    mix_copies, mix_turned = mix_parts(tp, sel, returned, out_cot)
    mixed = exchange(mix_turned, ("y", "core", "tp"))
    mix_grad = exchange(mix_copies, "tp")
    partial_proj = proj_partial(mixed, act_near)
    proj_grad = jnp.sum(exchange(partial_proj, "z").astype(f32), axis=0)

    mix_rows = jnp.moveaxis(mix_grad, 0, 1).reshape(tokens_here, model_width)
    norm_in_grad = dot(mix_rows, out_weight, 1, 1)
    scaled = norm_in_grad * sig_norm * (1.0 + normed * (1.0 - sig_norm)) * norm_gain[None, :]
    dot_sum = from_everyone(jnp.sum(conv_vals * scaled, axis=1)[None], "tp").sum(axis=(0, 1))
    conv_grad = inv_rms * scaled - conv_vals * inv_rms**3 * (dot_sum / model_width)[:, None]
    reach = conv_taps.shape[0] - 1
    route = [(i, i - 1) for i in range(1, experts)]
    following = lax.ppermute(conv_grad[:reach].astype(bf16), SP, route).astype(f32)
    extended = jnp.concatenate([conv_grad, following], axis=0)
    gated_grad = jnp.zeros((tokens_here, quarter), f32)
    for tap_index in range(reach + 1):
        gated_grad = (
            gated_grad
            + conv_taps[tap_index][None, :] * extended[tap_index : tap_index + tokens_here]
        )
    return (gate_g[None], up_g[None], down_g[None], proj_grad, gated_grad)


def solution(mesh):
    fine = Mesh(mesh.devices.reshape(8, 4, 2, 4), ("z", "y", "core", "tp"))
    placed = (
        P(SP, None),
        P(SP, "tp"),
        P(SP, None),
        P(SP, None),
        P(SP, None),
        P(SP, None, "tp"),
        P(SP, None, "tp"),
        P(SP, "tp", None),
        P("tp", None),
        P("tp"),
        P(None, "tp"),
    )
    return jax.shard_map(
        on_device,
        mesh=fine,
        in_specs=placed,
        out_specs=(
            P(SP, None, "tp"),
            P(SP, None, "tp"),
            P(SP, "tp", None),
            P(SP, "tp"),
            P(SP, "tp"),
        ),
        check_vma=False,
    )
```

```python
import jax
import jax.numpy as jnp
from jax import lax
from jax.experimental import pallas as pl
from jax.experimental.pallas import tpu as pltpu
from jax.sharding import Mesh
from jax.sharding import PartitionSpec as P


norm_epsilon = 1e-05
SP = ("z", "y", "core")
f32 = jnp.float32
bf16 = jnp.bfloat16
VM = pl.BlockSpec(memory_space=pltpu.VMEM)
SM = pl.BlockSpec(memory_space=pltpu.SMEM)


PARAMS = pltpu.CompilerParams(vmem_limit_bytes=20 * 2**20)


def cost(flops, moved):
    return pl.CostEstimate(flops=flops, bytes_accessed=moved, transcendentals=0)


def dot(a, b, ca, cb):
    return lax.dot_general(a, b, (((ca,), (cb,)), ((), ())), preferred_element_type=f32)


def send_kernel(tp_ref, routes_ref, weight_ref, x_ref, cot_ref, send_ref, sel_ref):
    tokens = routes_ref.shape[1]
    slots = sel_ref.shape[0]
    experts = send_ref.shape[0]
    capacity = slots // experts
    expert_row = lax.broadcasted_iota(jnp.int32, (experts, tokens), 0)
    earlier = (
        lax.broadcasted_iota(jnp.int32, (tokens, tokens), 0)
        < lax.broadcasted_iota(jnp.int32, (tokens, tokens), 1)
    ).astype(bf16)
    slot_row = lax.broadcasted_iota(jnp.int32, (slots, tokens), 0)
    total = jnp.zeros((experts, 1), f32)
    picks = []
    for k in range(routes_ref.shape[0]):
        named = routes_ref[k : k + 1, :]
        hot = (expert_row == named).astype(f32)
        before = dot(hot.astype(bf16), earlier, 1, 0) + total
        total = total + jnp.sum(hot, axis=1, keepdims=True)
        within = jnp.sum(hot * before, axis=0, keepdims=True).astype(jnp.int32)
        picks.append((slot_row == named * capacity + within).astype(bf16))
    both = picks[0] + picks[1]
    sel_ref[...] = both
    shape = (experts, capacity, x_ref.shape[1])
    send_ref[:, :, : shape[2]] = dot(both, x_ref[...], 1, 0).astype(bf16).reshape(shape)
    cot = cot_ref[...].astype(f32)
    weight = jnp.broadcast_to(weight_ref[0:1, :], (8, tokens)).T, jnp.broadcast_to(
        weight_ref[1:2, :], (8, tokens)
    ).T
    scaled = [(weight[k][:, 0:1] * cot).astype(bf16) for k in range(2)]
    out = dot(picks[0], scaled[0], 1, 0) + dot(picks[1], scaled[1], 1, 0)
    send_ref[:, :, shape[2] :] = out.astype(bf16).reshape(shape)


def send_rows(tp, routes, route_weight, mixer_out, out_cot, experts, capacity, quarter):
    tokens = out_cot.shape[0]
    column = pl.BlockSpec((tokens, quarter), lambda i, t: (0, t[0]))
    whole = lambda shape: pl.BlockSpec(shape, lambda i, t: (0,) * len(shape))
    sent = jax.ShapeDtypeStruct((experts, capacity, 2 * quarter), bf16)
    return pl.pallas_call(
        send_kernel,
        grid_spec=pltpu.PrefetchScalarGridSpec(
            num_scalar_prefetch=1,
            grid=(1,),
            in_specs=[whole((2, tokens)), whole((2, tokens)), column, column],
            out_specs=[whole(sent.shape), whole((experts * capacity, tokens))],
        ),
        out_shape=[sent, jax.ShapeDtypeStruct((experts * capacity, tokens), bf16)],
        cost_estimate=cost(400_000_000, 3_000_000),
    )(tp, routes.T, route_weight.T, mixer_out, out_cot)


def block_of(t, k):
    return lax.rem(t + k, 4)


def times(block_refs, w_ref, t, width, cw):
    acc = None
    for k in range(4):
        at = pl.ds(pl.multiple_of(block_of(t, k) * width, width), width)
        w = w_ref[at, :] if cw == 0 else w_ref[:, at]
        if k == 2:
            part = jnp.concatenate([dot(r[...], w, 1, cw) for r in block_refs[2:4]], axis=0)
        else:
            part = dot(block_refs[k + (k == 3)][...], w, 1, cw)
        acc = part if acc is None else acc + part
    return acc


def forward_kernel(t_ref, *refs):
    blocks, (wg_ref, wu_ref, pg_ref, pu_ref) = refs[:5], refs[5:]
    width = blocks[0].shape[1]
    pg_ref[...] = times(blocks, wg_ref, t_ref[0], width, 0)
    pu_ref[...] = times(blocks, wu_ref, t_ref[0], width, 0)


def expert_forward(tp, x_blocks, w_gate, w_up):
    rows, hidden = x_blocks[0].shape[0], w_gate.shape[1]
    out = jax.ShapeDtypeStruct((rows, hidden), f32)
    return pl.pallas_call(
        forward_kernel,
        in_specs=[SM] + [VM] * 7,
        out_specs=[VM, VM],
        out_shape=[out, out],
        compiler_params=PARAMS,
        cost_estimate=cost(1_073_741_824, 5_000_000),
    )(tp, *x_blocks, w_gate, w_up)


def backward_kernel(t_ref, *refs):
    blocks = refs[:5]
    wd_ref, pg_ref, pu_ref, wg_ref, wu_ref, act_ref, gp_ref, up_ref = refs[5:13]
    outs = refs[13:]
    width = blocks[0].shape[1]
    half = blocks[0].shape[0] // 2
    act_grad = times(blocks, wd_ref, t_ref[0], width, 1)
    pre_gate = pg_ref[...]
    pre_up = pu_ref[...]
    sig = jax.nn.sigmoid(pre_gate)
    silu = pre_gate * sig
    act_ref[...] = (silu * pre_up).astype(bf16)
    gp_ref[...] = (act_grad * pre_up * sig * (1.0 + pre_gate * (1.0 - sig))).astype(bf16)
    up_ref[...] = (act_grad * silu).astype(bf16)
    for i, k in enumerate((2, 3, 1, 0)):
        cols = pl.ds(pl.multiple_of(block_of(t_ref[0], k) * width, width), width)
        back = dot(gp_ref[...], wg_ref[cols, :], 1, 1) + dot(up_ref[...], wu_ref[cols, :], 1, 1)
        outs[2 * i][...] = back[:half].astype(bf16)
        outs[2 * i + 1][...] = back[half:].astype(bf16)


def expert_backward(tp, c_blocks, w_down, pre_gate, pre_up, w_gate, w_up):
    half, width = c_blocks[2].shape
    rows, hidden = pre_gate.shape
    small = jax.ShapeDtypeStruct((rows, hidden), bf16)
    return pl.pallas_call(
        backward_kernel,
        in_specs=[SM] + [VM] * 10,
        out_specs=[VM] * 11,
        out_shape=[small] * 3 + [jax.ShapeDtypeStruct((half, width), bf16)] * 8,
        compiler_params=PARAMS,
        cost_estimate=cost(1_610_612_736, 9_000_000),
    )(tp, *c_blocks, w_down, pre_gate, pre_up, w_gate, w_up)


def weight_kernel(t_ref, *refs):
    xs, cs = refs[:5], refs[5:10]
    act_ref, gp_ref, up_ref, gg_ref, ug_ref, dg_ref = refs[10:]
    _, width = xs[2].shape
    for k in range(4):
        at = pl.ds(pl.multiple_of(block_of(t_ref[0], k) * width, width), width)
        i = k + (k == 3)
        x, c = (
            jnp.concatenate([b[2][...], b[3][...]], axis=0) if k == 2 else b[i][...]
            for b in (xs, cs)
        )
        gg_ref[at, :] = dot(x, gp_ref[...], 0, 0).astype(bf16)
        ug_ref[at, :] = dot(x, up_ref[...], 0, 0).astype(bf16)
        dg_ref[:, at] = dot(act_ref[...], c, 0, 0).astype(bf16)


def weight_grads(tp, x_blocks, c_blocks, act, gate_pre, up_pre):
    width = x_blocks[0].shape[1]
    hidden = act.shape[1]
    tall = jax.ShapeDtypeStruct((4 * width, hidden), bf16)
    return pl.pallas_call(
        weight_kernel,
        in_specs=[SM] + [VM] * 13,
        out_specs=[VM] * 3,
        out_shape=[tall, tall, jax.ShapeDtypeStruct((hidden, 4 * width), bf16)],
        compiler_params=PARAMS,
        cost_estimate=cost(1_610_612_736, 8_000_000),
    )(tp, *x_blocks, *c_blocks, act, gate_pre, up_pre)


def column(row):
    return jnp.broadcast_to(row, (8, row.shape[1])).T[:, 0:1]


def gate(conv, inv_rms, gain):
    normed = conv * inv_rms * gain
    sig = jax.nn.sigmoid(normed)
    return normed * sig, sig * (1.0 + normed * (1.0 - sig)) * gain


def act_kernel(t_ref, p0_ref, p1_ref, p2_ref, p3_ref, conv_ref, gain_ref, w_ref, act_ref, inv_ref, *q_refs):
    width = conv_ref.shape[1]
    power = (p0_ref[...] + p1_ref[...]) + (p2_ref[...] + p3_ref[...])
    inv_rms = column(lax.rsqrt(power / w_ref.shape[1] + norm_epsilon))
    conv = conv_ref[...].astype(f32)
    act, slope = gate(conv, inv_rms, gain_ref[...])
    act_ref[...] = act.astype(bf16)
    inv_ref[...] = inv_rms
    pulled = (conv * slope).astype(bf16)
    for k in range(4):
        at = pl.ds(pl.multiple_of(block_of(t_ref[0], k) * width, width), width)
        q_refs[k][...] = dot(pulled, w_ref[:, at], 1, 0).astype(bf16)


def act_parts(tp, powers, conv_out, gain, out_weight):
    block = jax.ShapeDtypeStruct(conv_out.shape, bf16)
    return pl.pallas_call(
        act_kernel,
        in_specs=[SM] + [VM] * 7,
        out_specs=[VM] * 6,
        out_shape=[block, jax.ShapeDtypeStruct((conv_out.shape[0], 1), f32)] + [block] * 4,
        compiler_params=PARAMS,
        cost_estimate=cost(268_435_456, 3_000_000),
    )(tp, *powers, conv_out, gain, out_weight)


def mix_kernel(t_ref, sel_ref, back_ref, q_ref, cot_ref, mix_ref, out_ref, dot_ref):
    tokens, width = cot_ref.shape
    ret = back_ref[...].reshape(sel_ref.shape[0], width)
    mix = cot_ref[...].astype(f32) + dot(sel_ref[...], ret, 0, 0)
    mix_ref[...] = mix.astype(bf16)
    turned = mix.T.astype(bf16)
    run = width // 16
    for g in range(8):
        piece = jnp.concatenate(
            [turned[(q * 8 + g) * run : (q * 8 + g + 1) * run] for q in range(2)], axis=0
        )
        for j in range(4):
            out_ref[g * 4 + j] = piece
    dots = jnp.sum(mix.astype(bf16).astype(f32) * q_ref[...], axis=1, keepdims=True)
    dot_ref[...] = jnp.broadcast_to(dots, (tokens, 128)).T[0:1, :]


def mix_parts(tp, sel, returned, q_total, out_cot):
    tokens = out_cot.shape[0]
    _, _, quarter = returned.shape
    whole = lambda shape: pl.BlockSpec(shape, lambda i, t: (0,) * len(shape))
    shapes = [(tokens, quarter), (32, quarter // 8, tokens)]
    return pl.pallas_call(
        mix_kernel,
        grid_spec=pltpu.PrefetchScalarGridSpec(
            num_scalar_prefetch=1,
            grid=(1,),
            in_specs=[
                whole(sel.shape),
                whole(returned.shape),
                whole((tokens, quarter)),
                pl.BlockSpec((tokens, quarter), lambda i, t: (0, t[0])),
            ],
            out_specs=[*[whole(s) for s in shapes], whole((1, tokens))],
        ),
        out_shape=[
            *[jax.ShapeDtypeStruct(s, bf16) for s in shapes],
            jax.ShapeDtypeStruct((1, tokens), f32),
        ],
        compiler_params=PARAMS,
        cost_estimate=cost(70_000_000, 2_000_000),
    )(tp, sel, returned, q_total, out_cot)


def sum_kernel(oa_ref, na_ref, pa_ref, ob_ref, nb_ref, pb_ref, out_ref):
    half = out_ref.shape[0] // 2
    for at, refs in ((0, (oa_ref, na_ref, pa_ref)), (half, (ob_ref, nb_ref, pb_ref))):
        total = refs[0][...].astype(f32) + refs[1][...].astype(f32) + refs[2][...].astype(f32)
        out_ref[pl.ds(at, half)] = total.astype(bf16).reshape(half, *out_ref.shape[1:])


def sum_rows(parts, experts):
    rows, width = parts[0].shape
    shape = (experts, 2 * rows // experts, width)
    return pl.pallas_call(
        sum_kernel,
        in_specs=[VM] * 6,
        out_specs=VM,
        out_shape=jax.ShapeDtypeStruct(shape, bf16),
        compiler_params=PARAMS,
        cost_estimate=cost(1_000_000, 2_000_000),
    )(*parts)


def proj_kernel(at_ref, mix_ref, *refs):
    acts, (out_ref, left_ref, right_ref, sems) = refs[:4], refs[4:]
    rows, tokens = 4 * mix_ref.shape[1], mix_ref.shape[2]
    copies = []
    for r in range(4):
        for c in range(2):
            core = at_ref[1] if c == 0 else 1 - at_ref[1]
            g = 2 * block_of(at_ref[0], r) + core
            to = right_ref.at[pl.ds(pl.multiple_of(g * tokens, tokens), tokens)]
            copies.append(pltpu.make_async_copy(acts[r].at[c], to, sems.at[2 * r + c]))
    for copy in copies:
        copy.start()
    for g in range(8):
        left_ref[:, g * tokens : (g + 1) * tokens] = mix_ref[4 * g : 4 * g + 4].reshape(rows, tokens)
    for copy in copies:
        copy.wait()
    out = dot(left_ref[...], right_ref[...], 1, 0)
    out_ref[...] = out.astype(bf16).reshape(out_ref.shape)


def proj_partial(at, mixed, acts):
    tokens, width = acts[0].shape[1:]
    rows = 4 * mixed.shape[1]
    return pl.pallas_call(
        proj_kernel,
        in_specs=[SM, VM] + [pl.BlockSpec(memory_space=pltpu.HBM)] * 4,
        out_specs=VM,
        out_shape=jax.ShapeDtypeStruct((8, rows // 8, width), bf16),
        scratch_shapes=[
            pltpu.VMEM((rows, 8 * tokens), bf16),
            pltpu.VMEM((8 * tokens, width), bf16),
            pltpu.SemaphoreType.DMA((8,)),
        ],
        compiler_params=PARAMS,
        cost_estimate=cost(268_435_456, 2_000_000),
    )(at, mixed, *acts)


def grad_kernel(t_ref, *refs):
    blocks, dots = refs[:4], refs[4:8]
    inv_ref, conv_ref, gain_ref, w_ref, out_ref, head_ref = refs[8:]
    width = blocks[0].shape[1]
    back = None
    for k in range(4):
        at = pl.ds(pl.multiple_of(block_of(t_ref[0], k) * width, width), width)
        part = dot(blocks[k][...], w_ref[:, at], 1, 1)
        back = part if back is None else back + part
    conv = conv_ref[...].astype(f32)
    inv_rms = inv_ref[...]
    scaled = back * gate(conv, inv_rms, gain_ref[...])[1]
    total = (dots[0][...] + dots[1][...]) + (dots[2][...] + dots[3][...])
    pull = column(total / w_ref.shape[1]) * inv_rms * inv_rms * inv_rms
    conv_grad = inv_rms * scaled - conv * pull
    out_ref[...] = conv_grad
    head_ref[...] = conv_grad[: head_ref.shape[0]].astype(bf16)


def conv_backward(tp, blocks, dots, inv_rms, conv_out, gain, out_weight):
    return pl.pallas_call(
        grad_kernel,
        in_specs=[SM] + [VM] * 12,
        out_specs=[VM] * 2,
        out_shape=[
            jax.ShapeDtypeStruct(conv_out.shape, f32),
            jax.ShapeDtypeStruct((32, conv_out.shape[1]), bf16),
        ],
        compiler_params=PARAMS,
        cost_estimate=cost(268_435_456, 2_000_000),
    )(tp, *blocks, *dots, inv_rms, conv_out, gain, out_weight)


def taps_kernel(grad_ref, next_ref, taps_ref, out_ref, ext_ref):
    tokens, width = grad_ref.shape
    ext_ref[pl.ds(0, tokens), :] = grad_ref[...]
    ext_ref[pl.ds(tokens, next_ref.shape[0]), :] = next_ref[...].astype(f32)
    for lane in range(0, width, 128):
        lanes = pl.ds(lane, 128)
        acc = None
        for w in range(taps_ref.shape[0]):
            part = taps_ref[w : w + 1, lanes] * ext_ref[pl.ds(w, tokens), lanes]
            acc = part if acc is None else acc + part
        out_ref[:, lanes] = acc


def taps_backward(conv_grad, following, taps):
    rows = conv_grad.shape[0] + following.shape[0]
    return pl.pallas_call(
        taps_kernel,
        in_specs=[VM] * 3,
        out_specs=VM,
        out_shape=jax.ShapeDtypeStruct(conv_grad.shape, f32),
        scratch_shapes=[pltpu.VMEM((rows, conv_grad.shape[1]), f32)],
        compiler_params=PARAMS,
        cost_estimate=cost(4_000_000, 1_000_000),
    )(conv_grad, following, taps)


def exchange(x, axis):
    return lax.all_to_all(x, axis, split_axis=0, concat_axis=0, tiled=True)


AHEAD = [(i, (i + 1) % 4) for i in range(4)]
BEHIND = [(i, (i - 1) % 4) for i in range(4)]
ACROSS = [(i, (i + 2) % 4) for i in range(4)]


def ring_gather(block):
    half = block.shape[0] // 2
    ahead = lax.ppermute(block, "tp", AHEAD)
    behind = lax.ppermute(block, "tp", BEHIND)
    across_a = lax.ppermute(ahead[:half], "tp", AHEAD)
    across_b = lax.ppermute(behind[half:], "tp", BEHIND)
    return [block, behind, across_a, across_b, ahead]


def ring_all(x, axis="tp"):
    ahead = lax.ppermute(x, axis, AHEAD)
    behind = lax.ppermute(x, axis, BEHIND)
    across = lax.ppermute(x, axis, ACROSS)
    return [x, behind, across, ahead]


def plus(*terms):
    return sum(x.astype(f32) for x in terms).astype(bf16)


def ring_scatter(far_a, far_b, prev_a, prev_b, next_a, next_b, own_a, own_b):
    far_a = lax.ppermute(far_a, "tp", AHEAD)
    far_b = lax.ppermute(far_b, "tp", BEHIND)
    next_b = lax.ppermute(next_b, "tp", AHEAD)
    prev_a = lax.ppermute(prev_a, "tp", BEHIND)
    next_a = lax.ppermute(plus(next_a, far_a), "tp", AHEAD)
    prev_b = lax.ppermute(plus(prev_b, far_b), "tp", BEHIND)
    return own_a, next_a, prev_a, own_b, next_b, prev_b


def on_device(
    mixer_out,
    conv_out,
    out_cot,
    routes,
    route_weight,
    gate_weight,
    up_weight,
    down_weight,
    out_weight,
    norm_gain,
    conv_taps,
):
    tokens_here, _ = out_cot.shape
    experts = lax.axis_size(SP)
    capacity = 2 * tokens_here * routes.shape[1] // experts
    quarter = conv_out.shape[1]
    tp = lax.axis_index("tp").astype(jnp.int32)[None]
    w_gate, w_up, w_down = gate_weight[0], up_weight[0], down_weight[0]

    send, sel = send_rows(
        tp, routes, route_weight, mixer_out, out_cot, experts, capacity, quarter
    )
    slots = experts * capacity
    arrived = exchange(send, SP).reshape(slots, 2 * quarter)
    x_slice, cot_slice = arrived[:, :quarter], arrived[:, quarter:]

    conv_vals = conv_out.astype(f32)
    powers = ring_all(jnp.sum(conv_vals * conv_vals, axis=1)[None])
    gain = norm_gain[None]
    activated, inv_rms, *q_parts = act_parts(tp, powers, conv_out, gain, out_weight)
    q_ahead = lax.ppermute(q_parts[1], "tp", AHEAD)
    q_across = lax.ppermute(q_parts[2], "tp", ACROSS)
    q_behind = lax.ppermute(q_parts[3], "tp", BEHIND)
    q_total = sum(q.astype(f32) for q in (q_parts[0], q_ahead, q_across, q_behind))
    act_other = lax.ppermute(activated, "core", [(0, 1), (1, 0)])
    act_near = ring_all(jnp.stack([activated, act_other]), "y")

    x_blocks = ring_gather(x_slice)
    pre_gate, pre_up = expert_forward(tp, x_blocks, w_gate, w_up)
    c_blocks = ring_gather(cot_slice)
    act, gate_pre, up_pre, *parts = expert_backward(
        tp, c_blocks, w_down, pre_gate, pre_up, w_gate, w_up
    )
    sums = ring_scatter(*parts)
    back = sum_rows(sums, experts)
    returned = exchange(back, SP)
    gate_g, up_g, down_g = weight_grads(tp, x_blocks, c_blocks, act, gate_pre, up_pre)

    mix_part, mix_turned, dots = mix_parts(tp, sel, returned, q_total, out_cot)
    mixed = exchange(mix_turned, ("y", "core", "tp"))
    mix_blocks = ring_all(mix_part)
    at = jnp.stack([lax.axis_index("y"), lax.axis_index("core")]).astype(jnp.int32)
    partial_proj = proj_partial(at, mixed, act_near)
    partial_proj = exchange(partial_proj, "z")
    proj_grad = jnp.sum(partial_proj.astype(f32), axis=0)

    dot_blocks = ring_all(dots)
    conv_grad, head = conv_backward(
        tp, mix_blocks, dot_blocks, inv_rms, conv_out, gain, out_weight
    )
    route = [(i, i - 1) for i in range(1, experts)]
    following = lax.ppermute(head, SP, route)
    gated_grad = taps_backward(conv_grad, following, conv_taps)
    return (gate_g[None], up_g[None], down_g[None], proj_grad, gated_grad)


def solution(mesh):
    fine = Mesh(mesh.devices.reshape(8, 4, 2, 4), ("z", "y", "core", "tp"))
    placed = (
        P(SP, None),
        P(SP, "tp"),
        P(SP, None),
        P(SP, None),
        P(SP, None),
        P(SP, None, "tp"),
        P(SP, None, "tp"),
        P(SP, "tp", None),
        P("tp", None),
        P("tp"),
        P(None, "tp"),
    )
    return jax.shard_map(
        on_device,
        mesh=fine,
        in_specs=placed,
        out_specs=(
            P(SP, None, "tp"),
            P(SP, None, "tp"),
            P(SP, "tp", None),
            P(SP, "tp"),
            P(SP, "tp"),
        ),
        check_vma=False,
    )
```

```python
import jax
import jax.numpy as jnp
from jax import lax
from jax.experimental import pallas as pl
from jax.experimental.pallas import tpu as pltpu
from jax.sharding import Mesh
from jax.sharding import PartitionSpec as P


norm_epsilon = 1e-05
SP = ("z", "y", "core")
f32 = jnp.float32
bf16 = jnp.bfloat16
VM = pl.BlockSpec(memory_space=pltpu.VMEM)
SM = pl.BlockSpec(memory_space=pltpu.SMEM)


PARAMS = pltpu.CompilerParams(vmem_limit_bytes=20 * 2**20)


def cost(flops, moved):
    return pl.CostEstimate(flops=flops, bytes_accessed=moved, transcendentals=0)


def dot(a, b, ca, cb):
    return lax.dot_general(a, b, (((ca,), (cb,)), ((), ())), preferred_element_type=f32)


def send_kernel(tp_ref, routes_ref, weight_ref, x_ref, cot_ref, send_ref, sel_ref):
    tokens = routes_ref.shape[1]
    slots = sel_ref.shape[0]
    experts = send_ref.shape[0]
    capacity = slots // experts
    expert_row = lax.broadcasted_iota(jnp.int32, (experts, tokens), 0)
    earlier = (
        lax.broadcasted_iota(jnp.int32, (tokens, tokens), 0)
        < lax.broadcasted_iota(jnp.int32, (tokens, tokens), 1)
    ).astype(bf16)
    slot_row = lax.broadcasted_iota(jnp.int32, (slots, tokens), 0)
    total = jnp.zeros((experts, 1), f32)
    picks = []
    for k in range(routes_ref.shape[0]):
        named = routes_ref[k : k + 1, :]
        hot = (expert_row == named).astype(f32)
        before = dot(hot.astype(bf16), earlier, 1, 0) + total
        total = total + jnp.sum(hot, axis=1, keepdims=True)
        within = jnp.sum(hot * before, axis=0, keepdims=True).astype(jnp.int32)
        picks.append((slot_row == named * capacity + within).astype(bf16))
    both = picks[0] + picks[1]
    sel_ref[...] = both
    shape = (experts, capacity, x_ref.shape[1])
    send_ref[:, :, : shape[2]] = dot(both, x_ref[...], 1, 0).astype(bf16).reshape(shape)
    cot = cot_ref[...].astype(f32)
    weight = jnp.broadcast_to(weight_ref[0:1, :], (8, tokens)).T, jnp.broadcast_to(
        weight_ref[1:2, :], (8, tokens)
    ).T
    scaled = [(weight[k][:, 0:1] * cot).astype(bf16) for k in range(2)]
    out = dot(picks[0], scaled[0], 1, 0) + dot(picks[1], scaled[1], 1, 0)
    send_ref[:, :, shape[2] :] = out.astype(bf16).reshape(shape)


def send_rows(tp, routes, route_weight, mixer_out, out_cot, experts, capacity, quarter):
    tokens = out_cot.shape[0]
    column = pl.BlockSpec((tokens, quarter), lambda i, t: (0, t[0]))
    whole = lambda shape: pl.BlockSpec(shape, lambda i, t: (0,) * len(shape))
    sent = jax.ShapeDtypeStruct((experts, capacity, 2 * quarter), bf16)
    return pl.pallas_call(
        send_kernel,
        grid_spec=pltpu.PrefetchScalarGridSpec(
            num_scalar_prefetch=1,
            grid=(1,),
            in_specs=[whole((2, tokens)), whole((2, tokens)), column, column],
            out_specs=[whole(sent.shape), whole((experts * capacity, tokens))],
        ),
        out_shape=[sent, jax.ShapeDtypeStruct((experts * capacity, tokens), bf16)],
        cost_estimate=cost(400_000_000, 3_000_000),
    )(tp, routes.T, route_weight.T, mixer_out, out_cot)


def block_of(t, k):
    return lax.rem(t + k, 4)


def times(block_refs, w_ref, t, width, cw):
    acc = None
    for k in range(4):
        at = pl.ds(pl.multiple_of(block_of(t, k) * width, width), width)
        w = w_ref[at, :] if cw == 0 else w_ref[:, at]
        if k == 2:
            part = jnp.concatenate([dot(r[...], w, 1, cw) for r in block_refs[2:4]], axis=0)
        else:
            part = dot(block_refs[k + (k == 3)][...], w, 1, cw)
        acc = part if acc is None else acc + part
    return acc


def forward_kernel(t_ref, *refs):
    blocks, (wg_ref, wu_ref, pg_ref, pu_ref) = refs[:5], refs[5:]
    width = blocks[0].shape[1]
    pg_ref[...] = times(blocks, wg_ref, t_ref[0], width, 0)
    pu_ref[...] = times(blocks, wu_ref, t_ref[0], width, 0)


def expert_forward(tp, x_blocks, w_gate, w_up):
    rows, hidden = x_blocks[0].shape[0], w_gate.shape[1]
    out = jax.ShapeDtypeStruct((rows, hidden), f32)
    return pl.pallas_call(
        forward_kernel,
        in_specs=[SM] + [VM] * 7,
        out_specs=[VM, VM],
        out_shape=[out, out],
        compiler_params=PARAMS,
        cost_estimate=cost(1_073_741_824, 5_000_000),
    )(tp, *x_blocks, w_gate, w_up)


def backward_kernel(t_ref, *refs):
    blocks = refs[:5]
    wd_ref, pg_ref, pu_ref, wg_ref, wu_ref, act_ref, gp_ref, up_ref = refs[5:13]
    outs = refs[13:]
    width = blocks[0].shape[1]
    act_grad = times(blocks, wd_ref, t_ref[0], width, 1)
    pre_gate = pg_ref[...]
    pre_up = pu_ref[...]
    sig = jax.nn.sigmoid(pre_gate)
    silu = pre_gate * sig
    act_ref[...] = (silu * pre_up).astype(bf16)
    gp_ref[...] = (act_grad * pre_up * sig * (1.0 + pre_gate * (1.0 - sig))).astype(bf16)
    up_ref[...] = (act_grad * silu).astype(bf16)
    row_parts(t_ref[0], (2,), gp_ref, up_ref, wg_ref, wu_ref, outs)


def row_parts(t, order, gp_ref, up_ref, wg_ref, wu_ref, outs):
    half, width = outs[0].shape
    for i, k in enumerate(order):
        cols = pl.ds(pl.multiple_of(block_of(t, k) * width, width), width)
        back = dot(gp_ref[...], wg_ref[cols, :], 1, 1) + dot(up_ref[...], wu_ref[cols, :], 1, 1)
        outs[2 * i][...] = back[:half].astype(bf16)
        outs[2 * i + 1][...] = back[half:].astype(bf16)


def expert_backward(tp, c_blocks, w_down, pre_gate, pre_up, w_gate, w_up):
    half, width = c_blocks[2].shape
    rows, hidden = pre_gate.shape
    small = jax.ShapeDtypeStruct((rows, hidden), bf16)
    return pl.pallas_call(
        backward_kernel,
        in_specs=[SM] + [VM] * 10,
        out_specs=[VM] * 5,
        out_shape=[small] * 3 + [jax.ShapeDtypeStruct((half, width), bf16)] * 2,
        compiler_params=PARAMS,
        cost_estimate=cost(1_000_000_000, 6_000_000),
    )(tp, *c_blocks, w_down, pre_gate, pre_up, w_gate, w_up)


def rest_kernel(t_ref, gp_ref, up_ref, wg_ref, wu_ref, *outs):
    row_parts(t_ref[0], (3, 1, 0), gp_ref, up_ref, wg_ref, wu_ref, outs)


def rest_backward(tp, gate_pre, up_pre, w_gate, w_up):
    block = jax.ShapeDtypeStruct((gate_pre.shape[0] // 2, w_gate.shape[0] // 4), bf16)
    return pl.pallas_call(
        rest_kernel,
        in_specs=[SM] + [VM] * 4,
        out_specs=[VM] * 6,
        out_shape=[block] * 6,
        compiler_params=PARAMS,
        cost_estimate=cost(800_000_000, 4_000_000),
    )(tp, gate_pre, up_pre, w_gate, w_up)


def weight_kernel(t_ref, *refs):
    xs, cs = refs[:5], refs[5:10]
    act_ref, gp_ref, up_ref, gg_ref, ug_ref, dg_ref = refs[10:]
    _, width = xs[2].shape
    for k in range(4):
        at = pl.ds(pl.multiple_of(block_of(t_ref[0], k) * width, width), width)
        i = k + (k == 3)
        x, c = (
            jnp.concatenate([b[2][...], b[3][...]], axis=0) if k == 2 else b[i][...]
            for b in (xs, cs)
        )
        gg_ref[at, :] = dot(x, gp_ref[...], 0, 0).astype(bf16)
        ug_ref[at, :] = dot(x, up_ref[...], 0, 0).astype(bf16)
        dg_ref[:, at] = dot(act_ref[...], c, 0, 0).astype(bf16)


def weight_grads(tp, x_blocks, c_blocks, act, gate_pre, up_pre):
    width = x_blocks[0].shape[1]
    hidden = act.shape[1]
    tall = jax.ShapeDtypeStruct((4 * width, hidden), bf16)
    return pl.pallas_call(
        weight_kernel,
        in_specs=[SM] + [VM] * 13,
        out_specs=[VM] * 3,
        out_shape=[tall, tall, jax.ShapeDtypeStruct((hidden, 4 * width), bf16)],
        compiler_params=PARAMS,
        cost_estimate=cost(1_610_612_736, 8_000_000),
    )(tp, *x_blocks, *c_blocks, act, gate_pre, up_pre)


def column(row):
    return jnp.broadcast_to(row, (8, row.shape[1])).T[:, 0:1]


def gate(conv, inv_rms, gain):
    normed = conv * inv_rms * gain
    sig = jax.nn.sigmoid(normed)
    return normed * sig, sig * (1.0 + normed * (1.0 - sig)) * gain


def act_kernel(t_ref, p0_ref, p1_ref, p2_ref, p3_ref, conv_ref, gain_ref, w_ref, act_ref, inv_ref, *q_refs):
    width = conv_ref.shape[1]
    power = (p0_ref[...] + p1_ref[...]) + (p2_ref[...] + p3_ref[...])
    inv_rms = column(lax.rsqrt(power / w_ref.shape[1] + norm_epsilon))
    conv = conv_ref[...].astype(f32)
    act, slope = gate(conv, inv_rms, gain_ref[...])
    act_ref[...] = act.astype(bf16)
    inv_ref[...] = inv_rms
    pulled = (conv * slope).astype(bf16)
    for k in range(4):
        at = pl.ds(pl.multiple_of(block_of(t_ref[0], k) * width, width), width)
        q_refs[k][...] = dot(pulled, w_ref[:, at], 1, 0).astype(bf16)


def act_parts(tp, powers, conv_out, gain, out_weight):
    block = jax.ShapeDtypeStruct(conv_out.shape, bf16)
    return pl.pallas_call(
        act_kernel,
        in_specs=[SM] + [VM] * 7,
        out_specs=[VM] * 6,
        out_shape=[block, jax.ShapeDtypeStruct((conv_out.shape[0], 1), f32)] + [block] * 4,
        compiler_params=PARAMS,
        cost_estimate=cost(268_435_456, 3_000_000),
    )(tp, *powers, conv_out, gain, out_weight)


def mix_kernel(t_ref, sel_ref, back_ref, q_ref, cot_ref, mix_ref, out_ref, dot_ref):
    tokens, width = cot_ref.shape
    ret = back_ref[...].reshape(sel_ref.shape[0], width)
    mix = cot_ref[...].astype(f32) + dot(sel_ref[...], ret, 0, 0)
    mix_ref[...] = mix.astype(bf16)
    turned = mix.T.astype(bf16)
    run = width // 16
    for g in range(8):
        piece = jnp.concatenate(
            [turned[(q * 8 + g) * run : (q * 8 + g + 1) * run] for q in range(2)], axis=0
        )
        for j in range(4):
            out_ref[g * 4 + j] = piece
    dots = jnp.sum(mix.astype(bf16).astype(f32) * q_ref[...], axis=1, keepdims=True)
    dot_ref[...] = jnp.broadcast_to(dots, (tokens, 128)).T[0:1, :]


def mix_parts(tp, sel, returned, q_total, out_cot):
    tokens = out_cot.shape[0]
    _, _, quarter = returned.shape
    whole = lambda shape: pl.BlockSpec(shape, lambda i, t: (0,) * len(shape))
    shapes = [(tokens, quarter), (32, quarter // 8, tokens)]
    return pl.pallas_call(
        mix_kernel,
        grid_spec=pltpu.PrefetchScalarGridSpec(
            num_scalar_prefetch=1,
            grid=(1,),
            in_specs=[
                whole(sel.shape),
                whole(returned.shape),
                whole((tokens, quarter)),
                pl.BlockSpec((tokens, quarter), lambda i, t: (0, t[0])),
            ],
            out_specs=[*[whole(s) for s in shapes], whole((1, tokens))],
        ),
        out_shape=[
            *[jax.ShapeDtypeStruct(s, bf16) for s in shapes],
            jax.ShapeDtypeStruct((1, tokens), f32),
        ],
        compiler_params=PARAMS,
        cost_estimate=cost(70_000_000, 2_000_000),
    )(tp, sel, returned, q_total, out_cot)


def sum_kernel(oa_ref, na_ref, pa_ref, ob_ref, nb_ref, pb_ref, out_ref):
    half = out_ref.shape[0] // 2
    for at, refs in ((0, (oa_ref, na_ref, pa_ref)), (half, (ob_ref, nb_ref, pb_ref))):
        total = refs[0][...].astype(f32) + refs[1][...].astype(f32) + refs[2][...].astype(f32)
        out_ref[pl.ds(at, half)] = total.astype(bf16).reshape(half, *out_ref.shape[1:])


def sum_rows(parts, experts):
    rows, width = parts[0].shape
    shape = (experts, 2 * rows // experts, width)
    return pl.pallas_call(
        sum_kernel,
        in_specs=[VM] * 6,
        out_specs=VM,
        out_shape=jax.ShapeDtypeStruct(shape, bf16),
        compiler_params=PARAMS,
        cost_estimate=cost(1_000_000, 2_000_000),
    )(*parts)


def proj_kernel(at_ref, mix_ref, *refs):
    acts, out_ref = refs[:4], refs[4]
    rows, tokens = 4 * mix_ref.shape[1], mix_ref.shape[2]
    acc = None
    for r in range(4):
        first = 8 * block_of(at_ref[0], r)
        own, other = first + 4 * at_ref[1], first + 4 - 4 * at_ref[1]
        left = [mix_ref[pl.ds(g, 4)].reshape(rows, tokens) for g in (own, other)]
        right = acts[r][...].reshape(2 * tokens, acts[r].shape[2])
        part = dot(jnp.concatenate(left, axis=1), right, 1, 0)
        acc = part if acc is None else acc + part
    out_ref[...] = acc.astype(bf16).reshape(out_ref.shape)


def proj_partial(at, mixed, acts):
    width = acts[0].shape[2]
    return pl.pallas_call(
        proj_kernel,
        in_specs=[SM] + [VM] * 5,
        out_specs=VM,
        out_shape=jax.ShapeDtypeStruct((8, mixed.shape[1] // 2, width), bf16),
        compiler_params=PARAMS,
        cost_estimate=cost(268_435_456, 2_000_000),
    )(at, mixed, *acts)


def grad_kernel(t_ref, *refs):
    blocks, dots = refs[:4], refs[4:8]
    inv_ref, conv_ref, gain_ref, w_ref, out_ref, head_ref = refs[8:]
    width = blocks[0].shape[1]
    back = None
    for k in range(4):
        at = pl.ds(pl.multiple_of(block_of(t_ref[0], k) * width, width), width)
        part = dot(blocks[k][...], w_ref[:, at], 1, 1)
        back = part if back is None else back + part
    conv = conv_ref[...].astype(f32)
    inv_rms = inv_ref[...]
    scaled = back * gate(conv, inv_rms, gain_ref[...])[1]
    total = (dots[0][...] + dots[1][...]) + (dots[2][...] + dots[3][...])
    pull = column(total / w_ref.shape[1]) * inv_rms * inv_rms * inv_rms
    conv_grad = inv_rms * scaled - conv * pull
    out_ref[...] = conv_grad
    head_ref[...] = conv_grad[: head_ref.shape[0]].astype(bf16)


def conv_backward(tp, blocks, dots, inv_rms, conv_out, gain, out_weight):
    return pl.pallas_call(
        grad_kernel,
        in_specs=[SM] + [VM] * 12,
        out_specs=[VM] * 2,
        out_shape=[
            jax.ShapeDtypeStruct(conv_out.shape, f32),
            jax.ShapeDtypeStruct((32, conv_out.shape[1]), bf16),
        ],
        compiler_params=PARAMS,
        cost_estimate=cost(268_435_456, 2_000_000),
    )(tp, *blocks, *dots, inv_rms, conv_out, gain, out_weight)


def taps_kernel(grad_ref, next_ref, taps_ref, out_ref, ext_ref):
    tokens, width = grad_ref.shape
    ext_ref[pl.ds(0, tokens), :] = grad_ref[...]
    ext_ref[pl.ds(tokens, next_ref.shape[0]), :] = next_ref[...].astype(f32)
    for lane in range(0, width, 128):
        lanes = pl.ds(lane, 128)
        acc = None
        for w in range(taps_ref.shape[0]):
            part = taps_ref[w : w + 1, lanes] * ext_ref[pl.ds(w, tokens), lanes]
            acc = part if acc is None else acc + part
        out_ref[:, lanes] = acc


def taps_backward(conv_grad, following, taps):
    rows = conv_grad.shape[0] + following.shape[0]
    return pl.pallas_call(
        taps_kernel,
        in_specs=[VM] * 3,
        out_specs=VM,
        out_shape=jax.ShapeDtypeStruct(conv_grad.shape, f32),
        scratch_shapes=[pltpu.VMEM((rows, conv_grad.shape[1]), f32)],
        compiler_params=PARAMS,
        cost_estimate=cost(4_000_000, 1_000_000),
    )(conv_grad, following, taps)


def exchange(x, axis):
    return lax.all_to_all(x, axis, split_axis=0, concat_axis=0, tiled=True)


AHEAD = [(i, (i + 1) % 4) for i in range(4)]
BEHIND = [(i, (i - 1) % 4) for i in range(4)]
ACROSS = [(i, (i + 2) % 4) for i in range(4)]


def ring_gather(block):
    half = block.shape[0] // 2
    ahead = lax.ppermute(block, "tp", AHEAD)
    behind = lax.ppermute(block, "tp", BEHIND)
    across_a = lax.ppermute(ahead[:half], "tp", AHEAD)
    across_b = lax.ppermute(behind[half:], "tp", BEHIND)
    return [block, behind, across_a, across_b, ahead]


def ring_all(x, axis="tp"):
    ahead = lax.ppermute(x, axis, AHEAD)
    behind = lax.ppermute(x, axis, BEHIND)
    across = lax.ppermute(x, axis, ACROSS)
    return [x, behind, across, ahead]


def plus(*terms):
    return sum(x.astype(f32) for x in terms).astype(bf16)


def ring_scatter(far_a, far_b, prev_a, prev_b, next_a, next_b, own_a, own_b):
    far_a = lax.ppermute(far_a, "tp", AHEAD)
    far_b = lax.ppermute(far_b, "tp", BEHIND)
    next_b = lax.ppermute(next_b, "tp", AHEAD)
    prev_a = lax.ppermute(prev_a, "tp", BEHIND)
    next_a = lax.ppermute(plus(next_a, far_a), "tp", AHEAD)
    prev_b = lax.ppermute(plus(prev_b, far_b), "tp", BEHIND)
    return own_a, next_a, prev_a, own_b, next_b, prev_b


def on_device(
    mixer_out,
    conv_out,
    out_cot,
    routes,
    route_weight,
    gate_weight,
    up_weight,
    down_weight,
    out_weight,
    norm_gain,
    conv_taps,
):
    tokens_here, _ = out_cot.shape
    experts = lax.axis_size(SP)
    capacity = 2 * tokens_here * routes.shape[1] // experts
    quarter = conv_out.shape[1]
    tp = lax.axis_index("tp").astype(jnp.int32)[None]
    w_gate, w_up, w_down = gate_weight[0], up_weight[0], down_weight[0]

    send, sel = send_rows(
        tp, routes, route_weight, mixer_out, out_cot, experts, capacity, quarter
    )
    slots = experts * capacity
    arrived = exchange(send, SP).reshape(slots, 2 * quarter)
    x_slice, cot_slice = arrived[:, :quarter], arrived[:, quarter:]

    conv_vals = conv_out.astype(f32)
    powers = ring_all(jnp.sum(conv_vals * conv_vals, axis=1)[None])
    gain = norm_gain[None]
    activated, inv_rms, *q_parts = act_parts(tp, powers, conv_out, gain, out_weight)
    q_ahead = lax.ppermute(q_parts[1], "tp", AHEAD)
    q_across = lax.ppermute(q_parts[2], "tp", ACROSS)
    q_behind = lax.ppermute(q_parts[3], "tp", BEHIND)
    q_total = sum(q.astype(f32) for q in (q_parts[0], q_ahead, q_across, q_behind))
    act_other = lax.ppermute(activated, "core", [(0, 1), (1, 0)])
    act_near = ring_all(jnp.stack([activated, act_other]), "y")

    x_blocks = ring_gather(x_slice)
    pre_gate, pre_up = expert_forward(tp, x_blocks, w_gate, w_up)
    c_blocks = ring_gather(cot_slice)
    act, gate_pre, up_pre, *far = expert_backward(
        tp, c_blocks, w_down, pre_gate, pre_up, w_gate, w_up
    )
    rest = rest_backward(tp, gate_pre, up_pre, w_gate, w_up)
    sums = ring_scatter(*far, *rest)
    back = sum_rows(sums, experts)
    returned = exchange(back, SP)
    gate_g, up_g, down_g = weight_grads(tp, x_blocks, c_blocks, act, gate_pre, up_pre)

    mix_part, mix_turned, dots = mix_parts(tp, sel, returned, q_total, out_cot)
    mixed = exchange(mix_turned, ("y", "core", "tp"))
    mix_blocks = ring_all(mix_part)
    at = jnp.stack([lax.axis_index("y"), lax.axis_index("core")]).astype(jnp.int32)
    partial_proj = proj_partial(at, mixed, act_near)
    partial_proj = exchange(partial_proj, "z")
    proj_grad = jnp.sum(partial_proj.astype(f32), axis=0)

    dot_blocks = ring_all(dots)
    conv_grad, head = conv_backward(
        tp, mix_blocks, dot_blocks, inv_rms, conv_out, gain, out_weight
    )
    route = [(i, i - 1) for i in range(1, experts)]
    following = lax.ppermute(head, SP, route)
    gated_grad = taps_backward(conv_grad, following, conv_taps)
    return (gate_g[None], up_g[None], down_g[None], proj_grad, gated_grad)


def solution(mesh):
    fine = Mesh(mesh.devices.reshape(8, 4, 2, 4), ("z", "y", "core", "tp"))
    placed = (
        P(SP, None),
        P(SP, "tp"),
        P(SP, None),
        P(SP, None),
        P(SP, None),
        P(SP, None, "tp"),
        P(SP, None, "tp"),
        P(SP, "tp", None),
        P("tp", None),
        P("tp"),
        P(None, "tp"),
    )
    return jax.shard_map(
        on_device,
        mesh=fine,
        in_specs=placed,
        out_specs=(
            P(SP, None, "tp"),
            P(SP, None, "tp"),
            P(SP, "tp", None),
            P(SP, "tp"),
            P(SP, "tp"),
        ),
        check_vma=False,
    )
```

```python
import jax
import jax.numpy as jnp
from jax import lax
from jax.experimental import pallas as pl
from jax.experimental.pallas import tpu as pltpu
from jax.sharding import Mesh
from jax.sharding import PartitionSpec as P


norm_epsilon = 1e-05
SP = ("z", "y", "core")
f32 = jnp.float32
bf16 = jnp.bfloat16
VM = pl.BlockSpec(memory_space=pltpu.VMEM)
SM = pl.BlockSpec(memory_space=pltpu.SMEM)


PARAMS = pltpu.CompilerParams(vmem_limit_bytes=20 * 2**20)


def cost(flops, moved):
    return pl.CostEstimate(flops=flops, bytes_accessed=moved, transcendentals=0)


def dot(a, b, ca, cb):
    return lax.dot_general(a, b, (((ca,), (cb,)), ((), ())), preferred_element_type=f32)


def send_kernel(tp_ref, routes_ref, weight_ref, x_ref, cot_ref, send_ref, sel_ref):
    tokens = routes_ref.shape[1]
    slots = sel_ref.shape[0]
    experts = send_ref.shape[0]
    capacity = slots // experts
    expert_row = lax.broadcasted_iota(jnp.int32, (experts, tokens), 0)
    earlier = (
        lax.broadcasted_iota(jnp.int32, (tokens, tokens), 0)
        < lax.broadcasted_iota(jnp.int32, (tokens, tokens), 1)
    ).astype(bf16)
    slot_row = lax.broadcasted_iota(jnp.int32, (slots, tokens), 0)
    total = jnp.zeros((experts, 1), f32)
    picks = []
    for k in range(routes_ref.shape[0]):
        named = routes_ref[k : k + 1, :]
        hot = (expert_row == named).astype(f32)
        before = dot(hot.astype(bf16), earlier, 1, 0) + total
        total = total + jnp.sum(hot, axis=1, keepdims=True)
        within = jnp.sum(hot * before, axis=0, keepdims=True).astype(jnp.int32)
        picks.append((slot_row == named * capacity + within).astype(bf16))
    both = picks[0] + picks[1]
    sel_ref[...] = both
    shape = (experts, capacity, x_ref.shape[1])
    send_ref[:, :, : shape[2]] = dot(both, x_ref[...], 1, 0).astype(bf16).reshape(shape)
    cot = cot_ref[...].astype(f32)
    weight = jnp.broadcast_to(weight_ref[0:1, :], (8, tokens)).T, jnp.broadcast_to(
        weight_ref[1:2, :], (8, tokens)
    ).T
    scaled = [(weight[k][:, 0:1] * cot).astype(bf16) for k in range(2)]
    out = dot(jnp.concatenate(picks, axis=1), jnp.concatenate(scaled, axis=0), 1, 0)
    send_ref[:, :, shape[2] :] = out.astype(bf16).reshape(shape)


def send_rows(tp, routes, route_weight, mixer_out, out_cot, experts, capacity, quarter):
    tokens = out_cot.shape[0]
    column = pl.BlockSpec((tokens, quarter), lambda i, t: (0, t[0]))
    whole = lambda shape: pl.BlockSpec(shape, lambda i, t: (0,) * len(shape))
    sent = jax.ShapeDtypeStruct((experts, capacity, 2 * quarter), bf16)
    return pl.pallas_call(
        send_kernel,
        grid_spec=pltpu.PrefetchScalarGridSpec(
            num_scalar_prefetch=1,
            grid=(1,),
            in_specs=[whole((2, tokens)), whole((2, tokens)), column, column],
            out_specs=[whole(sent.shape), whole((experts * capacity, tokens))],
        ),
        out_shape=[sent, jax.ShapeDtypeStruct((experts * capacity, tokens), bf16)],
        cost_estimate=cost(400_000_000, 3_000_000),
    )(tp, routes.T, route_weight.T, mixer_out, out_cot)


def by_slice(w):
    return w.reshape(w.shape[0] // 32, 4, 8, w.shape[1])


def block_of(t, k):
    return lax.rem(t + k, 4)


def times(block_refs, w_ref, t, width, cw):
    acc = None
    for k in range(4):
        at = pl.ds(pl.multiple_of(block_of(t, k) * width, width), width)
        w = w_ref[at, :] if cw == 0 else w_ref[:, at]
        if k == 2:
            part = jnp.concatenate([dot(r[...], w, 1, cw) for r in block_refs[2:4]], axis=0)
        else:
            part = dot(block_refs[k + (k == 3)][...], w, 1, cw)
        acc = part if acc is None else acc + part
    return acc


def forward_kernel(t_ref, *refs):
    blocks, (wg_ref, wu_ref, pg_ref, pu_ref) = refs[:5], refs[5:]
    width = blocks[0].shape[1]
    pg_ref[...] = times(blocks, wg_ref, t_ref[0], width, 0)
    pu_ref[...] = times(blocks, wu_ref, t_ref[0], width, 0)


def expert_forward(tp, x_blocks, w_gate, w_up):
    rows, hidden = x_blocks[0].shape[0], w_gate.shape[1]
    out = jax.ShapeDtypeStruct((rows, hidden), f32)
    return pl.pallas_call(
        forward_kernel,
        in_specs=[SM] + [VM] * 7,
        out_specs=[VM, VM],
        out_shape=[out, out],
        compiler_params=PARAMS,
        cost_estimate=cost(1_073_741_824, 5_000_000),
    )(tp, *x_blocks, w_gate, w_up)


def backward_kernel(t_ref, *refs):
    blocks = refs[:5]
    wd_ref, pg_ref, pu_ref, wg_ref, wu_ref, act_ref, gp_ref, up_ref = refs[5:13]
    outs = refs[13:]
    width = blocks[0].shape[1]
    act_grad = times(blocks, wd_ref, t_ref[0], width, 1)
    pre_gate = pg_ref[...]
    pre_up = pu_ref[...]
    sig = jax.nn.sigmoid(pre_gate)
    silu = pre_gate * sig
    act_ref[...] = (silu * pre_up).astype(bf16)
    gp_ref[...] = (act_grad * pre_up * sig * (1.0 + pre_gate * (1.0 - sig))).astype(bf16)
    up_ref[...] = (act_grad * silu).astype(bf16)
    row_parts(t_ref[0], (2,), gp_ref, up_ref, wg_ref, wu_ref, outs)


def row_parts(t, order, gp_ref, up_ref, wg_ref, wu_ref, outs):
    half, width = outs[0].shape
    for i, k in enumerate(order):
        wg, wu = (w[:, block_of(t, k)].reshape(width, w.shape[3]) for w in (wg_ref, wu_ref))
        back = dot(gp_ref[...], wg, 1, 1) + dot(up_ref[...], wu, 1, 1)
        outs[2 * i][...] = back[:half].astype(bf16)
        outs[2 * i + 1][...] = back[half:].astype(bf16)


def expert_backward(tp, c_blocks, w_down, pre_gate, pre_up, w_gate, w_up):
    half, width = c_blocks[2].shape
    rows, hidden = pre_gate.shape
    small = jax.ShapeDtypeStruct((rows, hidden), bf16)
    return pl.pallas_call(
        backward_kernel,
        in_specs=[SM] + [VM] * 10,
        out_specs=[VM] * 5,
        out_shape=[small] * 3 + [jax.ShapeDtypeStruct((half, width), bf16)] * 2,
        compiler_params=PARAMS,
        cost_estimate=cost(1_000_000_000, 6_000_000),
    )(tp, *c_blocks, w_down, pre_gate, pre_up, w_gate, w_up)


def rest_kernel(t_ref, gp_ref, up_ref, wg_ref, wu_ref, *outs):
    row_parts(t_ref[0], (3, 1, 0), gp_ref, up_ref, wg_ref, wu_ref, outs)


def rest_backward(tp, gate_pre, up_pre, w_gate, w_up):
    block = jax.ShapeDtypeStruct((gate_pre.shape[0] // 2, w_gate.shape[0] * 8), bf16)
    return pl.pallas_call(
        rest_kernel,
        in_specs=[SM] + [VM] * 4,
        out_specs=[VM] * 6,
        out_shape=[block] * 6,
        compiler_params=PARAMS,
        cost_estimate=cost(800_000_000, 4_000_000),
    )(tp, gate_pre, up_pre, w_gate, w_up)


def weight_kernel(t_ref, *refs):
    xs, cs = refs[:5], refs[5:10]
    act_ref, gp_ref, up_ref, gg_ref, ug_ref, dg_ref = refs[10:]
    _, width = xs[2].shape
    step = 256

    @pl.loop(0, width // step)
    def _(h):
        lanes = pl.ds(pl.multiple_of(h * step, step), step)
        for k in range(4):
            first = block_of(t_ref[0], k) * width + h * step
            at = pl.ds(pl.multiple_of(first, step), step)
            i = k + (k == 3)
            x, c = (
                jnp.concatenate([b[2][:, lanes], b[3][:, lanes]], axis=0) if k == 2 else b[i][:, lanes]
                for b in (xs, cs)
            )
            gg_ref[at, :] = dot(x, gp_ref[...], 0, 0).astype(bf16)
            ug_ref[at, :] = dot(x, up_ref[...], 0, 0).astype(bf16)
            dg_ref[:, at] = dot(act_ref[...], c, 0, 0).astype(bf16)


def weight_grads(tp, x_blocks, c_blocks, act, gate_pre, up_pre):
    width = x_blocks[0].shape[1]
    hidden = act.shape[1]
    tall = jax.ShapeDtypeStruct((4 * width, hidden), bf16)
    return pl.pallas_call(
        weight_kernel,
        in_specs=[SM] + [VM] * 13,
        out_specs=[VM] * 3,
        out_shape=[tall, tall, jax.ShapeDtypeStruct((hidden, 4 * width), bf16)],
        compiler_params=PARAMS,
        cost_estimate=cost(1_610_612_736, 8_000_000),
    )(tp, *x_blocks, *c_blocks, act, gate_pre, up_pre)


def column(row):
    return jnp.broadcast_to(row, (8, row.shape[1])).T[:, 0:1]


def gate(conv, inv_rms, gain):
    normed = conv * inv_rms * gain
    sig = jax.nn.sigmoid(normed)
    return normed * sig, sig * (1.0 + normed * (1.0 - sig)) * gain


def act_kernel(t_ref, p0_ref, p1_ref, p2_ref, p3_ref, conv_ref, gain_ref, w_ref, cot_ref, act_ref, inv_ref, cott_ref, *q_refs):
    power = (p0_ref[...] + p1_ref[...]) + (p2_ref[...] + p3_ref[...])
    inv_rms = column(lax.rsqrt(power / w_ref.shape[1] + norm_epsilon))
    conv = conv_ref[...].astype(f32)
    act, slope = gate(conv, inv_rms, gain_ref[...])
    act_ref[...] = act.T.astype(bf16)
    inv_ref[...] = inv_rms
    q = dot((conv * slope).astype(bf16), w_ref[...], 1, 0).T
    q = q.reshape(q.shape[0] // 32, 4, 8, q.shape[1])
    scratch = q_refs[4]
    scratch[...] = q
    for k in range(4):
        q_refs[k][...] = scratch[:, block_of(t_ref[0], k)].astype(bf16)
    scratch[...] = cot_ref[...].astype(f32).T.reshape(q.shape)
    cott_ref[...] = scratch[:, t_ref[0]]


def act_parts(tp, powers, conv_out, gain, out_weight, out_cot):
    tokens, model_width = out_cot.shape
    block = jax.ShapeDtypeStruct((model_width // 32, 8, tokens), bf16)
    return pl.pallas_call(
        act_kernel,
        in_specs=[SM] + [VM] * 8,
        out_specs=[VM] * 7,
        out_shape=[
            jax.ShapeDtypeStruct((conv_out.shape[1], tokens), bf16),
            jax.ShapeDtypeStruct((tokens, 1), f32),
            jax.ShapeDtypeStruct(block.shape, f32),
            *[block] * 4,
        ],
        scratch_shapes=[pltpu.VMEM((model_width // 32, 4, 8, tokens), f32)],
        compiler_params=PARAMS,
        cost_estimate=cost(268_435_456, 3_000_000),
    )(tp, *powers, conv_out, gain, out_weight, out_cot)


def mix_kernel(at_ref, sel_ref, back_ref, q_ref, cot_ref, mix_ref, own_ref, other_ref, split_ref):
    slices, rows, tokens = cot_ref.shape
    ret = back_ref[...].reshape(sel_ref.shape[0], back_ref.shape[2])
    mix = (dot(ret, sel_ref[...], 0, 0).reshape(cot_ref.shape) + cot_ref[...]).astype(bf16)
    mix_ref[:slices] = mix
    split_ref[...] = mix.reshape(split_ref.shape)
    for r in range(4):
        to = 2 * block_of(at_ref[0], r)
        own_ref[r] = split_ref[:, to + at_ref[1]]
        other_ref[r] = split_ref[:, to + 1 - at_ref[1]]
    dots = mix.astype(f32) * q_ref[...]
    dots = jnp.sum(jnp.sum(dots, axis=0), axis=0, keepdims=True)
    high = dots.astype(bf16)
    low = (dots - high.astype(f32)).astype(bf16)
    row = lax.broadcasted_iota(jnp.int32, (rows, tokens), 0)
    pair = jnp.where(row == 0, high.astype(f32), jnp.where(row == 1, low.astype(f32), 0.0))
    mix_ref[slices] = pair.astype(bf16)


def mix_parts(at, sel, returned, q_total, cot_turned):
    slices, rows, tokens = cot_turned.shape
    near = jax.ShapeDtypeStruct((4, slices // 8, rows, tokens), bf16)
    return pl.pallas_call(
        mix_kernel,
        in_specs=[SM] + [VM] * 4,
        out_specs=[VM] * 3,
        out_shape=[jax.ShapeDtypeStruct((slices + 1, rows, tokens), bf16), near, near],
        scratch_shapes=[pltpu.VMEM((slices // 8, 8, rows, tokens), bf16)],
        compiler_params=PARAMS,
        cost_estimate=cost(70_000_000, 2_000_000),
    )(at, sel, returned, q_total, cot_turned)


def sum_kernel(oa_ref, na_ref, pa_ref, ob_ref, nb_ref, pb_ref, out_ref):
    half = out_ref.shape[0] // 2
    for at, refs in ((0, (oa_ref, na_ref, pa_ref)), (half, (ob_ref, nb_ref, pb_ref))):
        total = refs[0][...].astype(f32) + refs[1][...].astype(f32) + refs[2][...].astype(f32)
        out_ref[pl.ds(at, half)] = total.astype(bf16).reshape(half, *out_ref.shape[1:])


def sum_rows(parts, experts):
    rows, width = parts[0].shape
    shape = (experts, 2 * rows // experts, width)
    return pl.pallas_call(
        sum_kernel,
        in_specs=[VM] * 6,
        out_specs=VM,
        out_shape=jax.ShapeDtypeStruct(shape, bf16),
        compiler_params=PARAMS,
        cost_estimate=cost(1_000_000, 2_000_000),
    )(*parts)


def proj_kernel(at_ref, *refs):
    mixes, acts, out_ref = refs[:4], refs[4:8], refs[8]
    far, rows, tokens = mixes[0].shape[1:]
    width = out_ref.shape[3]
    right = [
        jnp.concatenate([m[c].reshape(far * rows, tokens) for c in range(2)], axis=1) for m in mixes
    ]

    @pl.loop(0, 4)
    def _(k):
        acc = None
        for r in range(4):
            left = jnp.concatenate([acts[r][c, k] for c in range(2)], axis=1)
            part = dot(left, right[r], 1, 1)
            acc = part if acc is None else acc + part
        out_ref[:, block_of(at_ref[2], k)] = acc.T.astype(bf16).reshape(far, rows, width)


def proj_partial(at, mixes, acts):
    _, far, rows, _ = mixes[0].shape
    return pl.pallas_call(
        proj_kernel,
        in_specs=[SM] + [VM] * 8,
        out_specs=VM,
        out_shape=jax.ShapeDtypeStruct((far, 4, rows, acts[0].shape[2]), bf16),
        compiler_params=PARAMS,
        cost_estimate=cost(268_435_456, 5_000_000),
    )(at, *mixes, *acts)


def grad_kernel(t_ref, *refs):
    blocks = refs[:4]
    inv_ref, conv_ref, gain_ref, w_ref, out_ref, head_ref, all_ref = refs[4:]
    slices = all_ref.shape[0]
    total = 0.0
    for k in range(4):
        all_ref[:, block_of(t_ref[0], k)] = blocks[k][:slices]
        total = total + jnp.sum(blocks[k][slices].astype(f32), axis=0, keepdims=True)
    back = dot(w_ref[...], all_ref[...].reshape(w_ref.shape[1], all_ref.shape[3]), 1, 0).T
    conv = conv_ref[...].astype(f32)
    inv_rms = inv_ref[...]
    scaled = back * gate(conv, inv_rms, gain_ref[...])[1]
    pull = column(total / w_ref.shape[1]) * inv_rms * inv_rms * inv_rms
    conv_grad = inv_rms * scaled - conv * pull
    out_ref[...] = conv_grad
    head_ref[...] = conv_grad[: head_ref.shape[0]].astype(bf16)


def conv_backward(tp, blocks, inv_rms, conv_out, gain, out_weight):
    return pl.pallas_call(
        grad_kernel,
        in_specs=[SM] + [VM] * 8,
        out_specs=[VM] * 2,
        out_shape=[
            jax.ShapeDtypeStruct(conv_out.shape, f32),
            jax.ShapeDtypeStruct((32, conv_out.shape[1]), bf16),
        ],
        scratch_shapes=[pltpu.VMEM((blocks[0].shape[0] - 1, 4, *blocks[0].shape[1:]), bf16)],
        compiler_params=PARAMS,
        cost_estimate=cost(268_435_456, 2_000_000),
    )(tp, *blocks, inv_rms, conv_out, gain, out_weight)


def taps_kernel(grad_ref, next_ref, taps_ref, out_ref, ext_ref):
    tokens, width = grad_ref.shape
    ext_ref[pl.ds(0, tokens), :] = grad_ref[...]
    ext_ref[pl.ds(tokens, next_ref.shape[0]), :] = next_ref[...].astype(f32)

    @pl.loop(0, width // 128)
    def _(lane):
        lanes = pl.ds(pl.multiple_of(lane * 128, 128), 128)
        acc = None
        for w in range(taps_ref.shape[0]):
            part = taps_ref[w : w + 1, lanes] * ext_ref[pl.ds(w, tokens), lanes]
            acc = part if acc is None else acc + part
        out_ref[:, lanes] = acc


def taps_backward(conv_grad, following, taps):
    rows = conv_grad.shape[0] + following.shape[0]
    return pl.pallas_call(
        taps_kernel,
        in_specs=[VM] * 3,
        out_specs=VM,
        out_shape=jax.ShapeDtypeStruct(conv_grad.shape, f32),
        scratch_shapes=[pltpu.VMEM((rows, conv_grad.shape[1]), f32)],
        compiler_params=PARAMS,
        cost_estimate=cost(4_000_000, 1_000_000),
    )(conv_grad, following, taps)


def exchange(x, axis):
    return lax.all_to_all(x, axis, split_axis=0, concat_axis=0, tiled=True)


AHEAD = [(i, (i + 1) % 4) for i in range(4)]
BEHIND = [(i, (i - 1) % 4) for i in range(4)]
ACROSS = [(i, (i + 2) % 4) for i in range(4)]


def ring_gather(block):
    half = block.shape[0] // 2
    ahead = lax.ppermute(block, "tp", AHEAD)
    behind = lax.ppermute(block, "tp", BEHIND)
    across_a = lax.ppermute(ahead[:half], "tp", AHEAD)
    across_b = lax.ppermute(behind[half:], "tp", BEHIND)
    return [block, behind, across_a, across_b, ahead]


def ring_all(x, axis="tp"):
    ahead = lax.ppermute(x, axis, AHEAD)
    behind = lax.ppermute(x, axis, BEHIND)
    across = lax.ppermute(x, axis, ACROSS)
    return [x, behind, across, ahead]


def plus(*terms):
    return sum(x.astype(f32) for x in terms).astype(bf16)


def ring_scatter(far_a, far_b, prev_a, prev_b, next_a, next_b, own_a, own_b):
    far_a = lax.ppermute(far_a, "tp", AHEAD)
    far_b = lax.ppermute(far_b, "tp", BEHIND)
    next_b = lax.ppermute(next_b, "tp", AHEAD)
    prev_a = lax.ppermute(prev_a, "tp", BEHIND)
    next_a = lax.ppermute(plus(next_a, far_a), "tp", AHEAD)
    prev_b = lax.ppermute(plus(prev_b, far_b), "tp", BEHIND)
    return own_a, next_a, prev_a, own_b, next_b, prev_b


def on_device(
    mixer_out,
    conv_out,
    out_cot,
    routes,
    route_weight,
    gate_weight,
    up_weight,
    down_weight,
    out_weight,
    norm_gain,
    conv_taps,
):
    tokens_here, _ = out_cot.shape
    experts = lax.axis_size(SP)
    capacity = 2 * tokens_here * routes.shape[1] // experts
    quarter = conv_out.shape[1]
    tp = lax.axis_index("tp").astype(jnp.int32)[None]
    w_gate, w_up, w_down = gate_weight[0], up_weight[0], down_weight[0]

    at = jnp.stack([lax.axis_index(a) for a in ("y", "core", "tp")]).astype(jnp.int32)
    send, sel = send_rows(tp, routes, route_weight, mixer_out, out_cot, experts, capacity, quarter)
    slots = experts * capacity
    arrived = exchange(send, SP).reshape(slots, 2 * quarter)
    x_slice, cot_slice = arrived[:, :quarter], arrived[:, quarter:]

    conv_vals = conv_out.astype(f32)
    powers = ring_all(jnp.sum(conv_vals * conv_vals, axis=1)[None])
    gain = norm_gain[None]
    activated, inv_rms, cot_turned, *q_parts = act_parts(
        tp, powers, conv_out, gain, out_weight, out_cot
    )
    q_ahead = lax.ppermute(q_parts[1], "tp", AHEAD)
    q_across = lax.ppermute(q_parts[2], "tp", ACROSS)
    q_behind = lax.ppermute(q_parts[3], "tp", BEHIND)
    q_total = sum(q.astype(f32) for q in (q_parts[0], q_ahead, q_across, q_behind))
    act_row = jnp.stack(ring_all(activated))
    act_other = lax.ppermute(act_row, "core", [(0, 1), (1, 0)])
    act_near = ring_all(jnp.stack([act_row, act_other]), "y")

    x_blocks = ring_gather(x_slice)
    pre_gate, pre_up = expert_forward(tp, x_blocks, w_gate, w_up)
    c_blocks = ring_gather(cot_slice)
    act, gate_pre, up_pre, *far = expert_backward(
        tp, c_blocks, w_down, pre_gate, pre_up, by_slice(w_gate), by_slice(w_up)
    )
    rest = rest_backward(tp, gate_pre, up_pre, by_slice(w_gate), by_slice(w_up))
    sums = ring_scatter(*far, *rest)
    back = sum_rows(sums, experts)
    returned = exchange(back, SP)
    gate_g, up_g, down_g = weight_grads(tp, x_blocks, c_blocks, act, gate_pre, up_pre)

    mix_part, mix_own, mix_other = mix_parts(at, sel, returned, q_total, cot_turned)
    mix_other = lax.ppermute(mix_other, "core", [(0, 1), (1, 0)])
    mix_pairs = jnp.stack([mix_own, mix_other], axis=1)
    mixes = [
        mix_pairs[0],
        lax.ppermute(mix_pairs[3], "y", BEHIND),
        lax.ppermute(mix_pairs[2], "y", ACROSS),
        lax.ppermute(mix_pairs[1], "y", AHEAD),
    ]
    mix_blocks = ring_all(mix_part)
    partial_proj = proj_partial(at, mixes, act_near)
    partial_proj = exchange(partial_proj.reshape(-1, *partial_proj.shape[2:]), ("z", "tp"))
    partial_proj = partial_proj.reshape(lax.axis_size("z"), -1, quarter)
    proj_grad = jnp.sum(partial_proj.astype(f32), axis=0)

    conv_grad, head = conv_backward(
        tp, mix_blocks, inv_rms, conv_out, gain, out_weight
    )
    route = [(i, i - 1) for i in range(1, experts)]
    following = lax.ppermute(head, SP, route)
    gated_grad = taps_backward(conv_grad, following, conv_taps)
    return (gate_g[None], up_g[None], down_g[None], proj_grad, gated_grad)


def solution(mesh):
    fine = Mesh(mesh.devices.reshape(8, 4, 2, 4), ("z", "y", "core", "tp"))
    placed = (
        P(SP, None),
        P(SP, "tp"),
        P(SP, None),
        P(SP, None),
        P(SP, None),
        P(SP, None, "tp"),
        P(SP, None, "tp"),
        P(SP, "tp", None),
        P("tp", None),
        P("tp"),
        P(None, "tp"),
    )
    return jax.shard_map(
        on_device,
        mesh=fine,
        in_specs=placed,
        out_specs=(
            P(SP, None, "tp"),
            P(SP, None, "tp"),
            P(SP, "tp", None),
            P(SP, "tp"),
            P(SP, "tp"),
        ),
        check_vma=False,
    )
```

```python
import jax
import jax.numpy as jnp
from jax import lax
from jax.experimental import pallas as pl
from jax.experimental.pallas import tpu as pltpu
from jax.sharding import Mesh
from jax.sharding import PartitionSpec as P


norm_epsilon = 1e-05
SP = ("z", "y", "core")
f32 = jnp.float32
bf16 = jnp.bfloat16
VM = pl.BlockSpec(memory_space=pltpu.VMEM)
SM = pl.BlockSpec(memory_space=pltpu.SMEM)


PARAMS = pltpu.CompilerParams(vmem_limit_bytes=20 * 2**20)


def cost(flops, moved):
    return pl.CostEstimate(flops=flops, bytes_accessed=moved, transcendentals=0)


def dot(a, b, ca, cb):
    return lax.dot_general(a, b, (((ca,), (cb,)), ((), ())), preferred_element_type=f32)


def send_kernel(tp_ref, routes_ref, weight_ref, x_ref, cot_ref, send_ref, sel_ref):
    tokens = routes_ref.shape[1]
    slots = sel_ref.shape[0]
    experts = send_ref.shape[0]
    capacity = slots // experts
    expert_row = lax.broadcasted_iota(jnp.int32, (experts, tokens), 0)
    earlier = (
        lax.broadcasted_iota(jnp.int32, (tokens, tokens), 0)
        < lax.broadcasted_iota(jnp.int32, (tokens, tokens), 1)
    ).astype(bf16)
    slot_row = lax.broadcasted_iota(jnp.int32, (slots, tokens), 0)
    total = jnp.zeros((experts, 1), f32)
    picks = []
    for k in range(routes_ref.shape[0]):
        named = routes_ref[k : k + 1, :]
        hot = (expert_row == named).astype(f32)
        before = dot(hot.astype(bf16), earlier, 1, 0) + total
        total = total + jnp.sum(hot, axis=1, keepdims=True)
        within = jnp.sum(hot * before, axis=0, keepdims=True).astype(jnp.int32)
        picks.append((slot_row == named * capacity + within).astype(bf16))
    both = picks[0] + picks[1]
    sel_ref[...] = both
    shape = (experts, capacity, x_ref.shape[1])
    send_ref[:, :, : shape[2]] = dot(both, x_ref[...], 1, 0).astype(bf16).reshape(shape)
    cot = cot_ref[...].astype(f32)
    weight = jnp.broadcast_to(weight_ref[0:1, :], (8, tokens)).T, jnp.broadcast_to(
        weight_ref[1:2, :], (8, tokens)
    ).T
    scaled = [(weight[k][:, 0:1] * cot).astype(bf16) for k in range(2)]
    out = dot(jnp.concatenate(picks, axis=1), jnp.concatenate(scaled, axis=0), 1, 0)
    send_ref[:, :, shape[2] :] = out.astype(bf16).reshape(shape)


def send_rows(tp, routes, route_weight, mixer_out, out_cot, experts, capacity, quarter):
    tokens = out_cot.shape[0]
    column = pl.BlockSpec((tokens, quarter), lambda i, t: (0, t[0]))
    whole = lambda shape: pl.BlockSpec(shape, lambda i, t: (0,) * len(shape))
    sent = jax.ShapeDtypeStruct((experts, capacity, 2 * quarter), bf16)
    return pl.pallas_call(
        send_kernel,
        grid_spec=pltpu.PrefetchScalarGridSpec(
            num_scalar_prefetch=1,
            grid=(1,),
            in_specs=[whole((2, tokens)), whole((2, tokens)), column, column],
            out_specs=[whole(sent.shape), whole((experts * capacity, tokens))],
        ),
        out_shape=[sent, jax.ShapeDtypeStruct((experts * capacity, tokens), bf16)],
        cost_estimate=cost(400_000_000, 3_000_000),
    )(tp, routes.T, route_weight.T, mixer_out, out_cot)


def by_slice(w):
    return w.reshape(w.shape[0] // 32, 4, 8, w.shape[1])


def block_of(t, k):
    return lax.rem(t + k, 4)


def times(block_refs, w_ref, t, width, cw):
    acc = None
    for k in range(4):
        at = pl.ds(pl.multiple_of(block_of(t, k) * width, width), width)
        w = w_ref[at, :] if cw == 0 else w_ref[:, at]
        if k == 2:
            part = jnp.concatenate([dot(r[...], w, 1, cw) for r in block_refs[2:4]], axis=0)
        else:
            part = dot(block_refs[k + (k == 3)][...], w, 1, cw)
        acc = part if acc is None else acc + part
    return acc


def forward_kernel(t_ref, *refs):
    blocks, (wg_ref, wu_ref, pg_ref, pu_ref) = refs[:5], refs[5:]
    width = blocks[0].shape[1]
    pg_ref[...] = times(blocks, wg_ref, t_ref[0], width, 0)
    pu_ref[...] = times(blocks, wu_ref, t_ref[0], width, 0)


def expert_forward(tp, x_blocks, w_gate, w_up):
    rows, hidden = x_blocks[0].shape[0], w_gate.shape[1]
    out = jax.ShapeDtypeStruct((rows, hidden), f32)
    return pl.pallas_call(
        forward_kernel,
        in_specs=[SM] + [VM] * 7,
        out_specs=[VM, VM],
        out_shape=[out, out],
        compiler_params=PARAMS,
        cost_estimate=cost(1_073_741_824, 5_000_000),
    )(tp, *x_blocks, w_gate, w_up)


def backward_kernel(t_ref, *refs):
    blocks = refs[:5]
    wd_ref, pg_ref, pu_ref, wg_ref, wu_ref, act_ref, gp_ref, up_ref = refs[5:13]
    outs = refs[13:]
    width = blocks[0].shape[1]
    act_grad = times(blocks, wd_ref, t_ref[0], width, 1)
    pre_gate = pg_ref[...]
    pre_up = pu_ref[...]
    sig = jax.nn.sigmoid(pre_gate)
    silu = pre_gate * sig
    act_ref[...] = (silu * pre_up).astype(bf16)
    gp_ref[...] = (act_grad * pre_up * sig * (1.0 + pre_gate * (1.0 - sig))).astype(bf16)
    up_ref[...] = (act_grad * silu).astype(bf16)
    row_parts(t_ref[0], (2,), gp_ref, up_ref, wg_ref, wu_ref, outs)


def row_parts(t, order, gp_ref, up_ref, wg_ref, wu_ref, outs):
    half, width = outs[0].shape
    for i, k in enumerate(order):
        wg, wu = (w[:, block_of(t, k)].reshape(width, w.shape[3]) for w in (wg_ref, wu_ref))
        back = dot(gp_ref[...], wg, 1, 1) + dot(up_ref[...], wu, 1, 1)
        outs[2 * i][...] = back[:half].astype(bf16)
        outs[2 * i + 1][...] = back[half:].astype(bf16)


def expert_backward(tp, c_blocks, w_down, pre_gate, pre_up, w_gate, w_up):
    half, width = c_blocks[2].shape
    rows, hidden = pre_gate.shape
    small = jax.ShapeDtypeStruct((rows, hidden), bf16)
    return pl.pallas_call(
        backward_kernel,
        in_specs=[SM] + [VM] * 10,
        out_specs=[VM] * 5,
        out_shape=[small] * 3 + [jax.ShapeDtypeStruct((half, width), bf16)] * 2,
        compiler_params=PARAMS,
        cost_estimate=cost(1_000_000_000, 6_000_000),
    )(tp, *c_blocks, w_down, pre_gate, pre_up, w_gate, w_up)


def rest_kernel(t_ref, gp_ref, up_ref, wg_ref, wu_ref, *outs):
    row_parts(t_ref[0], (3, 1, 0), gp_ref, up_ref, wg_ref, wu_ref, outs)


def rest_backward(tp, gate_pre, up_pre, w_gate, w_up):
    block = jax.ShapeDtypeStruct((gate_pre.shape[0] // 2, w_gate.shape[0] * 8), bf16)
    return pl.pallas_call(
        rest_kernel,
        in_specs=[SM] + [VM] * 4,
        out_specs=[VM] * 6,
        out_shape=[block] * 6,
        compiler_params=PARAMS,
        cost_estimate=cost(800_000_000, 4_000_000),
    )(tp, gate_pre, up_pre, w_gate, w_up)


def weight_kernel(t_ref, *refs):
    xs, cs = refs[:5], refs[5:10]
    act_ref, gp_ref, up_ref, gg_ref, ug_ref, dg_ref = refs[10:]
    _, width = xs[2].shape
    step = 256

    @pl.loop(0, width // step)
    def _(h):
        lanes = pl.ds(pl.multiple_of(h * step, step), step)
        for k in range(4):
            first = block_of(t_ref[0], k) * width + h * step
            at = pl.ds(pl.multiple_of(first, step), step)
            i = k + (k == 3)
            x, c = (
                jnp.concatenate([b[2][:, lanes], b[3][:, lanes]], axis=0) if k == 2 else b[i][:, lanes]
                for b in (xs, cs)
            )
            gg_ref[at, :] = dot(x, gp_ref[...], 0, 0).astype(bf16)
            ug_ref[at, :] = dot(x, up_ref[...], 0, 0).astype(bf16)
            dg_ref[:, at] = dot(act_ref[...], c, 0, 0).astype(bf16)


def weight_grads(tp, x_blocks, c_blocks, act, gate_pre, up_pre):
    width = x_blocks[0].shape[1]
    hidden = act.shape[1]
    tall = jax.ShapeDtypeStruct((4 * width, hidden), bf16)
    return pl.pallas_call(
        weight_kernel,
        in_specs=[SM] + [VM] * 13,
        out_specs=[VM] * 3,
        out_shape=[tall, tall, jax.ShapeDtypeStruct((hidden, 4 * width), bf16)],
        compiler_params=PARAMS,
        cost_estimate=cost(1_610_612_736, 8_000_000),
    )(tp, *x_blocks, *c_blocks, act, gate_pre, up_pre)


def column(row):
    return jnp.broadcast_to(row, (8, row.shape[1])).T[:, 0:1]


def gate(conv, inv_rms, gain):
    normed = conv * inv_rms * gain
    sig = jax.nn.sigmoid(normed)
    return normed * sig, sig * (1.0 + normed * (1.0 - sig)) * gain


def act_kernel(t_ref, p0_ref, p1_ref, p2_ref, p3_ref, conv_ref, gain_ref, w_ref, cot_ref, act_ref, inv_ref, cott_ref, *q_refs):
    power = (p0_ref[...] + p1_ref[...]) + (p2_ref[...] + p3_ref[...])
    inv_rms = column(lax.rsqrt(power / w_ref.shape[1] + norm_epsilon))
    conv = conv_ref[...].astype(f32)
    act, slope = gate(conv, inv_rms, gain_ref[...])
    act_ref[...] = act.T.astype(bf16)
    inv_ref[...] = inv_rms
    q = dot((conv * slope).astype(bf16), w_ref[...], 1, 0).T
    q = q.reshape(q.shape[0] // 32, 4, 8, q.shape[1])
    scratch = q_refs[4]
    scratch[...] = q
    for k in range(4):
        q_refs[k][...] = scratch[:, block_of(t_ref[0], k)].astype(bf16)
    scratch[...] = cot_ref[...].astype(f32).T.reshape(q.shape)
    cott_ref[...] = scratch[:, t_ref[0]]


def act_parts(tp, powers, conv_out, gain, out_weight, out_cot):
    tokens, model_width = out_cot.shape
    block = jax.ShapeDtypeStruct((model_width // 32, 8, tokens), bf16)
    return pl.pallas_call(
        act_kernel,
        in_specs=[SM] + [VM] * 8,
        out_specs=[VM] * 7,
        out_shape=[
            jax.ShapeDtypeStruct((conv_out.shape[1], tokens), bf16),
            jax.ShapeDtypeStruct((tokens, 1), f32),
            jax.ShapeDtypeStruct(block.shape, f32),
            *[block] * 4,
        ],
        scratch_shapes=[pltpu.VMEM((model_width // 32, 4, 8, tokens), f32)],
        compiler_params=PARAMS,
        cost_estimate=cost(268_435_456, 3_000_000),
    )(tp, *powers, conv_out, gain, out_weight, out_cot)


def mix_kernel(at_ref, sel_ref, back_ref, q_ref, cot_ref, mix_ref, own_ref, other_ref, split_ref):
    slices, rows, tokens = cot_ref.shape
    ret = back_ref[...].reshape(sel_ref.shape[0], back_ref.shape[2])
    mix = (dot(ret, sel_ref[...], 0, 0).reshape(cot_ref.shape) + cot_ref[...]).astype(bf16)
    mix_ref[:slices] = mix
    split_ref[...] = mix.reshape(split_ref.shape)
    for r in range(4):
        to = 2 * block_of(at_ref[0], r)
        own_ref[r] = split_ref[:, to + at_ref[1]]
        other_ref[r] = split_ref[:, to + 1 - at_ref[1]]
    dots = mix.astype(f32) * q_ref[...]
    dots = jnp.sum(jnp.sum(dots, axis=0), axis=0, keepdims=True)
    high = dots.astype(bf16)
    low = (dots - high.astype(f32)).astype(bf16)
    row = lax.broadcasted_iota(jnp.int32, (rows, tokens), 0)
    pair = jnp.where(row == 0, high.astype(f32), jnp.where(row == 1, low.astype(f32), 0.0))
    mix_ref[slices] = pair.astype(bf16)


def mix_parts(at, sel, returned, q_total, cot_turned):
    slices, rows, tokens = cot_turned.shape
    near = jax.ShapeDtypeStruct((4, slices // 8, rows, tokens), bf16)
    return pl.pallas_call(
        mix_kernel,
        in_specs=[SM] + [VM] * 4,
        out_specs=[VM] * 3,
        out_shape=[jax.ShapeDtypeStruct((slices + 1, rows, tokens), bf16), near, near],
        scratch_shapes=[pltpu.VMEM((slices // 8, 8, rows, tokens), bf16)],
        compiler_params=PARAMS,
        cost_estimate=cost(70_000_000, 2_000_000),
    )(at, sel, returned, q_total, cot_turned)


def sum_kernel(oa_ref, na_ref, pa_ref, ob_ref, nb_ref, pb_ref, out_ref):
    half = out_ref.shape[0] // 2
    for at, refs in ((0, (oa_ref, na_ref, pa_ref)), (half, (ob_ref, nb_ref, pb_ref))):
        total = refs[0][...].astype(f32) + refs[1][...].astype(f32) + refs[2][...].astype(f32)
        out_ref[pl.ds(at, half)] = total.astype(bf16).reshape(half, *out_ref.shape[1:])


def sum_rows(parts, experts):
    rows, width = parts[0].shape
    shape = (experts, 2 * rows // experts, width)
    return pl.pallas_call(
        sum_kernel,
        in_specs=[VM] * 6,
        out_specs=VM,
        out_shape=jax.ShapeDtypeStruct(shape, bf16),
        compiler_params=PARAMS,
        cost_estimate=cost(1_000_000, 2_000_000),
    )(*parts)


def proj_kernel(at_ref, *refs):
    mixes, acts, out_ref = refs[:4], refs[4:8], refs[8]
    far, rows, tokens = mixes[0].shape[1:]
    width = out_ref.shape[3]
    right = [
        jnp.concatenate([m[c].reshape(far * rows, tokens) for c in range(2)], axis=1) for m in mixes
    ]

    @pl.loop(0, 4)
    def _(k):
        acc = None
        for r in range(4):
            left = jnp.concatenate([acts[r][c, k] for c in range(2)], axis=1)
            part = dot(left, right[r], 1, 1)
            acc = part if acc is None else acc + part
        out_ref[:, block_of(at_ref[2], k)] = acc.T.astype(bf16).reshape(far, rows, width)


def proj_partial(at, mixes, acts):
    _, far, rows, _ = mixes[0].shape
    return pl.pallas_call(
        proj_kernel,
        in_specs=[SM] + [VM] * 8,
        out_specs=VM,
        out_shape=jax.ShapeDtypeStruct((far, 4, rows, acts[0].shape[2]), bf16),
        compiler_params=PARAMS,
        cost_estimate=cost(268_435_456, 5_000_000),
    )(at, *mixes, *acts)


def grad_kernel(t_ref, *refs):
    blocks = refs[:4]
    inv_ref, conv_ref, gain_ref, w_ref, out_ref, head_ref, all_ref = refs[4:]
    slices = all_ref.shape[0]
    total = 0.0
    for k in range(4):
        all_ref[:, block_of(t_ref[0], k)] = blocks[k][:slices]
        total = total + jnp.sum(blocks[k][slices].astype(f32), axis=0, keepdims=True)
    back = dot(w_ref[...], all_ref[...].reshape(w_ref.shape[1], all_ref.shape[3]), 1, 0).T
    conv = conv_ref[...].astype(f32)
    inv_rms = inv_ref[...]
    scaled = back * gate(conv, inv_rms, gain_ref[...])[1]
    pull = column(total / w_ref.shape[1]) * inv_rms * inv_rms * inv_rms
    conv_grad = inv_rms * scaled - conv * pull
    out_ref[...] = conv_grad
    head_ref[...] = conv_grad[: head_ref.shape[0]].astype(bf16)


def conv_backward(tp, blocks, inv_rms, conv_out, gain, out_weight):
    return pl.pallas_call(
        grad_kernel,
        in_specs=[SM] + [VM] * 8,
        out_specs=[VM] * 2,
        out_shape=[
            jax.ShapeDtypeStruct(conv_out.shape, f32),
            jax.ShapeDtypeStruct((32, conv_out.shape[1]), bf16),
        ],
        scratch_shapes=[pltpu.VMEM((blocks[0].shape[0] - 1, 4, *blocks[0].shape[1:]), bf16)],
        compiler_params=PARAMS,
        cost_estimate=cost(268_435_456, 2_000_000),
    )(tp, *blocks, inv_rms, conv_out, gain, out_weight)


def taps_kernel(grad_ref, next_ref, taps_ref, out_ref, ext_ref):
    tokens, width = grad_ref.shape
    ext_ref[pl.ds(0, tokens), :] = grad_ref[...]
    ext_ref[pl.ds(tokens, next_ref.shape[0]), :] = next_ref[...].astype(f32)

    @pl.loop(0, width // 128)
    def _(lane):
        lanes = pl.ds(pl.multiple_of(lane * 128, 128), 128)
        acc = None
        for w in range(taps_ref.shape[0]):
            part = taps_ref[w : w + 1, lanes] * ext_ref[pl.ds(w, tokens), lanes]
            acc = part if acc is None else acc + part
        out_ref[:, lanes] = acc


def taps_backward(conv_grad, following, taps):
    rows = conv_grad.shape[0] + following.shape[0]
    return pl.pallas_call(
        taps_kernel,
        in_specs=[VM] * 3,
        out_specs=VM,
        out_shape=jax.ShapeDtypeStruct(conv_grad.shape, f32),
        scratch_shapes=[pltpu.VMEM((rows, conv_grad.shape[1]), f32)],
        compiler_params=PARAMS,
        cost_estimate=cost(4_000_000, 1_000_000),
    )(conv_grad, following, taps)


def exchange(x, axis):
    return lax.all_to_all(x, axis, split_axis=0, concat_axis=0, tiled=True)


AHEAD = [(i, (i + 1) % 4) for i in range(4)]
BEHIND = [(i, (i - 1) % 4) for i in range(4)]
ACROSS = [(i, (i + 2) % 4) for i in range(4)]


def ring_gather(block):
    half = block.shape[0] // 2
    ahead = lax.ppermute(block, "tp", AHEAD)
    behind = lax.ppermute(block, "tp", BEHIND)
    across_a = lax.ppermute(ahead[:half], "tp", AHEAD)
    across_b = lax.ppermute(behind[half:], "tp", BEHIND)
    return [block, behind, across_a, across_b, ahead]


def ring_all(x, axis="tp"):
    ahead = lax.ppermute(x, axis, AHEAD)
    behind = lax.ppermute(x, axis, BEHIND)
    across = lax.ppermute(x, axis, ACROSS)
    return [x, behind, across, ahead]


def plus(*terms):
    return sum(x.astype(f32) for x in terms).astype(bf16)


def ring_scatter(far_a, far_b, prev_a, prev_b, next_a, next_b, own_a, own_b):
    far_a = lax.ppermute(far_a, "tp", AHEAD)
    far_b = lax.ppermute(far_b, "tp", BEHIND)
    next_b = lax.ppermute(next_b, "tp", AHEAD)
    prev_a = lax.ppermute(prev_a, "tp", BEHIND)
    next_a = lax.ppermute(plus(next_a, far_a), "tp", AHEAD)
    prev_b = lax.ppermute(plus(prev_b, far_b), "tp", BEHIND)
    return own_a, next_a, prev_a, own_b, next_b, prev_b


def on_device(
    mixer_out,
    conv_out,
    out_cot,
    routes,
    route_weight,
    gate_weight,
    up_weight,
    down_weight,
    out_weight,
    norm_gain,
    conv_taps,
):
    tokens_here, _ = out_cot.shape
    experts = lax.axis_size(SP)
    capacity = 2 * tokens_here * routes.shape[1] // experts
    quarter = conv_out.shape[1]
    tp = lax.axis_index("tp").astype(jnp.int32)[None]
    w_gate, w_up, w_down = gate_weight[0], up_weight[0], down_weight[0]

    at = jnp.stack([lax.axis_index(a) for a in ("y", "core", "tp")]).astype(jnp.int32)
    send, sel = send_rows(tp, routes, route_weight, mixer_out, out_cot, experts, capacity, quarter)
    slots = experts * capacity
    arrived = exchange(send, SP).reshape(slots, 2 * quarter)
    x_slice, cot_slice = arrived[:, :quarter], arrived[:, quarter:]

    conv_vals = conv_out.astype(f32)
    powers = ring_all(jnp.sum(conv_vals * conv_vals, axis=1)[None])
    gain = norm_gain[None]
    activated, inv_rms, cot_turned, *q_parts = act_parts(
        tp, powers, conv_out, gain, out_weight, out_cot
    )
    q_ahead = lax.ppermute(q_parts[1], "tp", AHEAD)
    q_across = lax.ppermute(q_parts[2], "tp", ACROSS)
    q_behind = lax.ppermute(q_parts[3], "tp", BEHIND)
    q_total = sum(q.astype(f32) for q in (q_parts[0], q_ahead, q_across, q_behind))
    act_row = jnp.stack(ring_all(activated))
    act_other = lax.ppermute(act_row, "core", [(0, 1), (1, 0)])
    act_near = ring_all(jnp.stack([act_row, act_other]), "y")

    x_blocks = ring_gather(x_slice)
    pre_gate, pre_up = expert_forward(tp, x_blocks, w_gate, w_up)
    c_blocks = ring_gather(cot_slice)
    act, gate_pre, up_pre, *far = expert_backward(
        tp, c_blocks, w_down, pre_gate, pre_up, by_slice(w_gate), by_slice(w_up)
    )
    rest = rest_backward(tp, gate_pre, up_pre, by_slice(w_gate), by_slice(w_up))
    sums = ring_scatter(*far, *rest)
    back = sum_rows(sums, experts)
    returned = exchange(back, SP)
    gate_g, up_g, down_g = weight_grads(tp, x_blocks, c_blocks, act, gate_pre, up_pre)

    mix_part, mix_own, mix_other = mix_parts(at, sel, returned, q_total, cot_turned)
    mix_other = lax.ppermute(mix_other, "core", [(0, 1), (1, 0)])
    mix_pairs = jnp.stack([mix_own, mix_other], axis=1)
    mixes = [
        mix_pairs[0],
        lax.ppermute(mix_pairs[3], "y", BEHIND),
        lax.ppermute(mix_pairs[2], "y", ACROSS),
        lax.ppermute(mix_pairs[1], "y", AHEAD),
    ]
    mix_ahead = lax.ppermute(mix_part, "tp", AHEAD)
    mix_behind = lax.ppermute(mix_part, "tp", BEHIND)
    mix_across = lax.ppermute(mix_part, "tp", ACROSS)
    mix_blocks = [mix_part, mix_behind, mix_across, mix_ahead]
    partial_proj = proj_partial(at, mixes, act_near)
    partial_proj = exchange(partial_proj.reshape(-1, *partial_proj.shape[2:]), ("z", "tp"))
    partial_proj = partial_proj.reshape(lax.axis_size("z"), -1, quarter)
    proj_grad = jnp.sum(partial_proj.astype(f32), axis=0)

    conv_grad, head = conv_backward(
        tp, mix_blocks, inv_rms, conv_out, gain, out_weight
    )
    route = [(i, i - 1) for i in range(1, experts)]
    following = lax.ppermute(head, SP, route)
    gated_grad = taps_backward(conv_grad, following, conv_taps)
    return (gate_g[None], up_g[None], down_g[None], proj_grad, gated_grad)


def solution(mesh):
    fine = Mesh(mesh.devices.reshape(8, 4, 2, 4), ("z", "y", "core", "tp"))
    placed = (
        P(SP, None),
        P(SP, "tp"),
        P(SP, None),
        P(SP, None),
        P(SP, None),
        P(SP, None, "tp"),
        P(SP, None, "tp"),
        P(SP, "tp", None),
        P("tp", None),
        P("tp"),
        P(None, "tp"),
    )
    return jax.shard_map(
        on_device,
        mesh=fine,
        in_specs=placed,
        out_specs=(
            P(SP, None, "tp"),
            P(SP, None, "tp"),
            P(SP, "tp", None),
            P(SP, "tp"),
            P(SP, "tp"),
        ),
        check_vma=False,
    )
```
